32 devices in a mesh: ep: 8 (over z, x), tp: 4 (over y, core).
Axes of the slice: x: 2, y: 2, z: 4, core: 2. Of those that a mesh axis runs over, the one named last changes fastest.
Arguments:
- queries: bfloat16 [4096, 1024], P('ep', 'tp'), may hold values from -8 to 8
- keys_values: bfloat16 [4096, 1024], P('ep', 'tp'), may hold values from -60 to 60
- forget_cache: float32 [16, 4096], P('tp'), may hold values from -617 to 0, as said below
- heads_gain: float32 [1024], replicated, may hold values from 0.1 to 1.9
- output_weight: bfloat16 [1024, 2048], replicated, may hold values from -0.1875 to 0.1875
- expert_tokens: bfloat16 [1024, 2048], P('ep'), may hold values from -600 to 600
- expert_gain: float32 [2048], replicated, may hold values from 0.1 to 1.9
- routes: int32 [1024, 4], P('ep'), may hold values from 0 to 7, all different within a row; in each aligned block of 128 rows (0 to 127, 128 to 255, ...) at most 128 rows name the same one
- route_logits: float32 [1024, 4], P('ep'), may hold values from -6 to 301
- gate_weight: bfloat16 [8, 2048, 2048], P('ep', None, 'tp'), may hold values from -0.5 to 0.5
- up_weight: bfloat16 [8, 2048, 2048], P('ep', None, 'tp'), may hold values from -0.5 to 0.5
- down_weight: bfloat16 [8, 2048, 2048], P('ep', 'tp'), may hold values from -0.015625 to 0.015625
Outputs:
- mixer_out: bfloat16 [4096, 2048], P(('ep', 'tp'))
- moe_out: bfloat16 [1024, 2048], P('ep', 'tp')
The draws below stay inside these ranges and needn't reach their ends.
Inputs may be any that keep to these rules, and one draw needn't show every extreme that they name: `forget_cache`: each row never rises from one position to the next. `routes`: the 4 experts of a row differ. In each aligned block of 128 rows (one device's tokens) no expert is named more than 128 times, so slot is below 128; some expert is named exactly 128 times in some block.
All inputs are finite; a program needn't handle non-finite values.
Results may differ from the reference program's by a relative error of at most 0.017.
Values may be sent and summed in bfloat16 or wider, within the bound.
A program may use at most 128 MiB of HBM per device.

```python
import math
import jax
import jax.numpy as jnp
import numpy as np
from jax import lax

D = 2048
ASKER_HEAD_TOTAL = 16
KV_HEADS = 8
HEAD = 64
FF = 2048
TOPK = 4
ATT_ROWS = 512
EXP_ROWS = 128
EXPERTS = 8
CAP = 128
MIXER_SEQ_SPAN = 4096
TOK_EXP = 1024
N_EP = 8
N_TP = 4


def base_values(key, shape):
    return jax.random.truncated_normal(key, -6.0, 6.0, shape, jnp.float32)


def draw_queries(key, part):
    result = base_values(jax.random.fold_in(key, 1), (MIXER_SEQ_SPAN, ASKER_HEAD_TOTAL, HEAD))
    return result.reshape(MIXER_SEQ_SPAN, ASKER_HEAD_TOTAL * HEAD).astype(jnp.bfloat16)


def draw_keys_values(key, part):
    key_rows = base_values(jax.random.fold_in(key, 2), (MIXER_SEQ_SPAN, KV_HEADS, HEAD))
    value_rows = base_values(jax.random.fold_in(key, 3), (MIXER_SEQ_SPAN, KV_HEADS, HEAD))
    scale_top = math.log(10.0)
    spread = jnp.exp(jax.random.uniform(jax.random.fold_in(key, 4), (1, KV_HEADS, HEAD), jnp.float32, 0.0, scale_top))
    value_rows = value_rows * spread
    joined = jnp.concatenate([key_rows, value_rows], axis=2)
    return joined.reshape(MIXER_SEQ_SPAN, KV_HEADS * 2 * HEAD).astype(jnp.bfloat16)


def draw_forget_cache(key, part):
    head_order = jax.random.permutation(jax.random.fold_in(key, 5), ASKER_HEAD_TOTAL)
    fast_heads = head_order < ASKER_HEAD_TOTAL // 2
    slow_rate = jnp.exp(jax.random.uniform(jax.random.fold_in(key, 6), (ASKER_HEAD_TOTAL,), jnp.float32, math.log(0.2), math.log(0.6))) / MIXER_SEQ_SPAN
    fast_rate = jnp.exp(jax.random.uniform(jax.random.fold_in(key, 7), (ASKER_HEAD_TOTAL,), jnp.float32, math.log(0.01), math.log(1.0 / 30.0)))
    step_rate = jnp.where(fast_heads, fast_rate, slow_rate)
    blocks = jnp.exp(jax.random.uniform(jax.random.fold_in(key, 8), (MIXER_SEQ_SPAN // ATT_ROWS,), jnp.float32, math.log(0.4), math.log(2.5)))
    per_block = jnp.repeat(blocks, ATT_ROWS)
    jitter = jax.random.uniform(jax.random.fold_in(key, 9), (ASKER_HEAD_TOTAL, MIXER_SEQ_SPAN), jnp.float32, 0.2, 1.8)
    decay_log_steps = step_rate[:, None] * per_block[None, :] * jitter
    decay_span_offset = jax.random.randint(jax.random.fold_in(key, 10), (ASKER_HEAD_TOTAL, 2), 0, MIXER_SEQ_SPAN)
    decay_span_size = jax.random.uniform(jax.random.fold_in(key, 12), (ASKER_HEAD_TOTAL, 2), jnp.float32, 0.22, 0.69)
    sequence_slot_number = jnp.arange(MIXER_SEQ_SPAN, dtype=jnp.int32)
    for decay_span_values in range(2):
        decay_log_steps = decay_log_steps + jnp.where(sequence_slot_number[None, :] == decay_span_offset[:, decay_span_values:decay_span_values + 1], decay_span_size[:, decay_span_values:decay_span_values + 1], 0.0)
    return -jnp.cumsum(decay_log_steps, axis=1)


def draw_expert_tokens(key, part):
    scale_top = math.log(10.0)
    result = base_values(jax.random.fold_in(key, 13), (TOK_EXP, D))
    row_scale = jnp.exp(jax.random.uniform(jax.random.fold_in(key, 14), (TOK_EXP, 1), jnp.float32, 0.0, math.log(10.0)))
    column_scale = jnp.exp(jax.random.uniform(jax.random.fold_in(key, 15), (1, D), jnp.float32, 0.0, scale_top))
    return (result * row_scale * column_scale).astype(jnp.bfloat16)


def draw_route_logits(key, part):
    result = base_values(jax.random.fold_in(key, 16), (TOK_EXP, TOPK))
    return result


def steps_of(stream_key, extent, shards, least, high):
    def one(dim, parts):
        heights = jax.random.uniform(jax.random.fold_in(jax.random.fold_in(stream_key, 6), dim), (parts,), jnp.float32, least / len(shards), high / len(shards))
        return jnp.repeat(jnp.exp(heights), extent[dim] // parts).reshape((-1,) + (1,) * (len(extent) - dim - 1))

    factor_of = one(*shards[0])
    for cut in shards[1:]:
        factor_of = factor_of * one(*cut)
    return factor_of


def deal_out(own_key, own, number, rows, count, top, limit, skew):
    sequence = jax.random.permutation(own_key, count)
    heavy_load, common = portions_of(count, rows * top, limit, skew, True), portions_of(count, rows * top, limit, skew, False)
    places = jnp.arange(count)

    def named(sizes, turn):
        used = int((sizes > 0).sum())
        fixed = max(1, used // 4)
        passed = fixed + (places - fixed + turn * (used - fixed)) % max(1, count - fixed)
        return jnp.zeros((count,), jnp.int32).at[sequence[jnp.where(places < fixed, places, passed)]].set(jnp.asarray(sizes, jnp.int32))

    sizes = jnp.where(number % 4 == 0, named(heavy_load, number // 4), named(common, number - number // 4 - 1))
    mixed = jax.random.permutation(jax.random.fold_in(own, 3), count)
    source_of, taker = mixed[0:count // 2 * 2:2], mixed[1:count // 2 * 2:2]
    slack = jnp.minimum(sizes[source_of] - 1, limit - sizes[taker]) // 2
    slack = jnp.where((source_of == sequence[0]) | (taker == sequence[0]) | (sizes[taker] == 0), 0, jnp.maximum(slack, 0))
    passed = jax.random.randint(jax.random.fold_in(own, 4), (count // 2,), 0, 1 << 20) % (slack + 1)
    sizes = sizes.at[source_of].add(-passed).at[taker].add(passed)
    items = jnp.searchsorted(jnp.cumsum(sizes), jnp.arange(rows * top), side="right").astype(jnp.int32)
    listing = items.reshape(top, rows).T
    listing = listing[jax.random.permutation(jax.random.fold_in(own, 1), rows)]
    turn = jax.random.randint(jax.random.fold_in(own, 2), (rows, 1), 0, top)
    return jnp.take_along_axis(listing, (jnp.arange(top)[None, :] + turn) % top, axis=1)


def portions_of(amount, total, bound, skew, full):
    portions = [(1 << 20) // math.isqrt(rank ** skew) + 1 for rank in range(1, amount + 1)]
    largest = bound if full else min(bound, max(-(-total // amount), total * portions[0] // sum(portions)))
    least = 1 if total - largest >= amount - 1 else 0
    given, surplus = [largest] + [least] * (amount - 1), total - largest - least * (amount - 1)
    while surplus > 0:
        movable = [i for i in range(1, amount) if given[i] < largest] or [i for i in range(1, amount) if given[i] < bound]
        whole, remaining = sum([portions[i] for i in movable]), surplus
        for i in movable:
            extra = min(bound - given[i], max(1, remaining * portions[i] // whole), surplus)
            given[i] = given[i] + extra
            surplus = surplus - extra
    return np.array(given)


def noise(own_key, dims, deviation, most, cuts=(), held_as=jnp.bfloat16):
    loudness = steps_of(own_key, dims, cuts, -0.22, 0.18) if cuts else 1.0
    values = jax.random.normal(own_key, dims, jnp.float32) * deviation * loudness
    return jnp.minimum(jnp.maximum(values, -most), most).astype(held_as)


def setup_inputs(seed: int = 0) -> dict:
    streams_of = jax.random.split(jax.random.key(seed), 13)
    queries = draw_queries(jax.random.fold_in(streams_of[12], 71), 0)
    keys_values = draw_keys_values(jax.random.fold_in(streams_of[12], 71), 0)
    forget_cache = draw_forget_cache(jax.random.fold_in(streams_of[12], 71), 0)
    heads_gain = jnp.clip(1.0 + 0.18 * jax.random.normal(streams_of[3], (ASKER_HEAD_TOTAL * HEAD,), jnp.float32), 0.1, 1.9)
    output_weight = noise(streams_of[4], (ASKER_HEAD_TOTAL * HEAD, D), (ASKER_HEAD_TOTAL * HEAD) ** -0.5, 0.1875)
    expert_tokens = draw_expert_tokens(jax.random.fold_in(streams_of[12], 71), 0)
    expert_gain = jnp.clip(1.0 + 0.18 * jax.random.normal(streams_of[6], (D,), jnp.float32), 0.1, 1.9)
    routes_keys = jax.random.split(jax.random.fold_in(streams_of[7], 1), TOK_EXP // EXP_ROWS)
    routes_turns = jax.random.permutation(jax.random.fold_in(streams_of[7], 3), TOK_EXP // EXP_ROWS)
    routes = jax.vmap(lambda own, number: deal_out(jax.random.fold_in(streams_of[7], 2), own, number, EXP_ROWS, EXPERTS, TOPK, CAP, 2))(routes_keys, routes_turns).reshape((TOK_EXP, TOPK))
    route_logits = draw_route_logits(jax.random.fold_in(streams_of[12], 71), 0)
    gate_weight = noise(streams_of[9], (EXPERTS, D, FF), (D // 16) ** -0.5, 0.5, ((0, 8), (2, 4)))
    up_weight = noise(streams_of[10], (EXPERTS, D, FF), (D // 16) ** -0.5, 0.5, ((0, 8), (2, 4)))
    down_weight = noise(streams_of[11], (EXPERTS, FF, D), (FF * 64) ** -0.5, 0.015625, ((0, 8), (1, 4)))
    return {"queries": queries, "keys_values": keys_values, "forget_cache": forget_cache, "heads_gain": heads_gain, "output_weight": output_weight, "expert_tokens": expert_tokens, "expert_gain": expert_gain, "routes": routes, "route_logits": route_logits, "gate_weight": gate_weight, "up_weight": up_weight, "down_weight": down_weight}


epsilon = 1e-06
clamp_limit = 7.0
sigmoid_slope = 1.702

def scaled_rows(values, gain_vector):
    as_float = values.astype(jnp.float32)
    inverse = lax.rsqrt(lax.optimization_barrier(jnp.mean(as_float * as_float, axis=-1, keepdims=True)) + epsilon)
    return (as_float * inverse * gain_vector.astype(jnp.float32)).astype(jnp.bfloat16)

def assign_slots(routes, experts, capacity):
    row_count, pick_count = routes.shape
    flat_routes = routes.reshape(-1)
    onehot = (flat_routes[:, None] == jnp.arange(experts, dtype=jnp.int32)[None, :]).astype(jnp.int32)
    earlier = jnp.cumsum(onehot, axis=0) - onehot
    slot_rank = lax.optimization_barrier(jnp.sum(earlier * onehot, axis=1)).astype(jnp.int32)
    position = (flat_routes * capacity + slot_rank).astype(jnp.int32)
    owner_row = (jnp.arange(row_count * pick_count, dtype=jnp.int32) // pick_count).astype(jnp.int32)
    slot_token = jnp.full((experts * capacity,), row_count, jnp.int32).at[position].set(owner_row)
    return (position.reshape(row_count, pick_count), slot_token)

def reference(queries, keys_values, forget_cache, heads_gain, output_weight, expert_tokens, expert_gain, routes, route_logits, gate_weight, up_weight, down_weight):
    group_size = ASKER_HEAD_TOTAL // KV_HEADS
    key_pairs = keys_values.reshape(MIXER_SEQ_SPAN, KV_HEADS, 2 * HEAD)
    query_heads = queries.reshape(MIXER_SEQ_SPAN, ASKER_HEAD_TOTAL, HEAD)
    block_width = math.gcd(MIXER_SEQ_SPAN, 512)
    key_pos = jnp.arange(MIXER_SEQ_SPAN, dtype=jnp.int32)
    score_scale = 1.0 / math.sqrt(HEAD)

    def one_head(head_number):
        key_head = head_number // group_size
        key_rows = key_pairs[:, key_head, :HEAD]
        value_rows = key_pairs[:, key_head, HEAD:]
        gate_row = forget_cache[head_number]
        query_all = query_heads[:, head_number, :]

        def one_block(block_index):
            first_row = block_index * block_width
            query_rows = lax.dynamic_slice_in_dim(query_all, first_row, block_width, 0)
            query_gate = lax.dynamic_slice_in_dim(gate_row, first_row, block_width, 0)
            scores = jnp.dot(query_rows, key_rows.T, preferred_element_type=jnp.float32) * score_scale
            scores = scores + query_gate[:, None] - gate_row[None, :]
            query_pos = first_row + jnp.arange(block_width, dtype=jnp.int32)
            scores = jnp.where(key_pos[None, :] <= query_pos[:, None], scores, -jnp.inf)
            row_max = lax.optimization_barrier(jnp.max(scores, axis=1, keepdims=True))
            weights = jnp.exp(scores - row_max)
            denominator = lax.optimization_barrier(jnp.sum(weights, axis=1, keepdims=True))
            summed = jnp.dot(weights.astype(jnp.bfloat16), value_rows, preferred_element_type=jnp.float32)
            return (summed / denominator).astype(jnp.bfloat16)
        return lax.map(one_block, jnp.arange(MIXER_SEQ_SPAN // block_width, dtype=jnp.int32)).reshape(MIXER_SEQ_SPAN, HEAD)
    attended = lax.map(one_head, jnp.arange(ASKER_HEAD_TOTAL, dtype=jnp.int32))
    attended = jnp.transpose(attended, (1, 0, 2)).reshape(MIXER_SEQ_SPAN, ASKER_HEAD_TOTAL * HEAD)
    heads_normed = scaled_rows(attended, heads_gain)
    mixer_out = jnp.dot(heads_normed, output_weight, preferred_element_type=jnp.float32).astype(jnp.bfloat16)
    expert_in = scaled_rows(expert_tokens, expert_gain)
    shifted = route_logits - lax.optimization_barrier(jnp.max(route_logits, axis=1, keepdims=True))
    raised = jnp.exp(shifted)
    route_weight = raised / lax.optimization_barrier(jnp.sum(raised, axis=1, keepdims=True))
    block_routes = routes.reshape(N_EP, EXP_ROWS, TOPK)
    block_weights = route_weight.reshape(N_EP, EXP_ROWS, TOPK)
    position, slot_token = jax.vmap(lambda chosen: assign_slots(chosen, EXPERTS, CAP))(block_routes)
    block_base = (jnp.arange(N_EP, dtype=jnp.int32) * EXP_ROWS)[:, None]
    global_token = jnp.where(slot_token < EXP_ROWS, slot_token + block_base, TOK_EXP).astype(jnp.int32)

    def weight_table(place, weights):
        return jnp.zeros((EXPERTS * CAP,), jnp.float32).at[place.reshape(-1)].set(weights.reshape(-1))
    slot_weight = jax.vmap(weight_table)(position, block_weights)
    padded = jnp.concatenate([expert_in, jnp.zeros((1, D), jnp.bfloat16)], axis=0)
    ff_block = FF // N_TP

    def accumulate(combined, expert):
        token_index = lax.dynamic_slice_in_dim(global_token, expert * CAP, CAP, 1).reshape(-1)
        slot_scale = lax.dynamic_slice_in_dim(slot_weight, expert * CAP, CAP, 1).reshape(-1)
        rows_in = jnp.take(padded, token_index, axis=0)
        gate_pre = jnp.dot(rows_in, gate_weight[expert], preferred_element_type=jnp.float32)
        up_pre = jnp.dot(rows_in, up_weight[expert], preferred_element_type=jnp.float32)
        gate_cut = jnp.minimum(gate_pre, clamp_limit)
        up_cut = jnp.clip(up_pre, -clamp_limit, clamp_limit)
        hidden = ((up_cut + 1.0) * gate_cut * jax.nn.sigmoid(sigmoid_slope * gate_cut)).astype(jnp.bfloat16)
        down_local = down_weight[expert]
        expert_sum = jnp.zeros((N_EP * CAP, D), jnp.float32)
        for block_index in range(N_TP):
            partial_value = jnp.dot(hidden[:, block_index * ff_block:(block_index + 1) * ff_block], down_local[block_index * ff_block:(block_index + 1) * ff_block, :], preferred_element_type=jnp.float32).astype(jnp.bfloat16)
            expert_sum = expert_sum + partial_value.astype(jnp.float32)
        expert_out = expert_sum.astype(jnp.bfloat16)
        combined = combined.at[token_index].add(expert_out.astype(jnp.float32) * slot_scale[:, None])
        return (combined, None)
    combined, _ = lax.scan(accumulate, jnp.zeros((TOK_EXP + 1, D), jnp.float32), jnp.arange(EXPERTS, dtype=jnp.int32))
    moe_out = combined[:TOK_EXP].astype(jnp.bfloat16)
    return (mixer_out, moe_out)
```

```python
import math

import jax
import jax.numpy as jnp
from jax import lax
from jax.experimental import pallas as pl
from jax.experimental.pallas import tpu as pltpu
from jax.sharding import PartitionSpec as P

HEAD = 64


epsilon = 1e-06
clamp_limit = 7.0
sigmoid_slope = 1.702


def scaled_rows(values, gain_vector):
    as_float = values.astype(jnp.float32)
    inverse = lax.rsqrt(jnp.mean(as_float * as_float, axis=-1, keepdims=True) + epsilon)
    return (as_float * inverse * gain_vector).astype(jnp.bfloat16)


def assign_slots(routes, experts, capacity):
    row_count, pick_count = routes.shape
    flat_routes = routes.reshape(-1)
    onehot = (flat_routes[:, None] == jnp.arange(experts, dtype=jnp.int32)[None, :]).astype(
        jnp.int32
    )
    earlier = jnp.cumsum(onehot, axis=0) - onehot
    slot_rank = jnp.sum(earlier * onehot, axis=1)
    position = flat_routes * capacity + slot_rank
    owner_row = jnp.arange(row_count * pick_count, dtype=jnp.int32) // pick_count
    slot_token = jnp.full((experts * capacity,), row_count, jnp.int32).at[position].set(owner_row)
    return (position.reshape(row_count, pick_count), slot_token)


def body(
    queries,
    keys_values,
    forget_cache,
    heads_gain,
    output_weight,
    expert_tokens,
    expert_gain,
    routes,
    route_logits,
    gate_weight,
    up_weight,
    down_weight,
):
    row_count = queries.shape[0]
    query_count = queries.shape[1] // HEAD
    key_count = keys_values.shape[1] // (2 * HEAD)
    group_size = query_count // key_count
    offset = lax.axis_index("ep") * row_count
    score_scale = 1.0 / math.sqrt(HEAD)
    count_rows = queries.shape[0]
    segment_positions = offset + jnp.arange(count_rows, dtype=jnp.int32)
    gate_rows = lax.dynamic_slice_in_dim(forget_cache, offset, count_rows, 1)
    segment_bias = gate_rows.T.reshape(count_rows, key_count, group_size, 1)
    segments = [
        (queries.reshape(count_rows, key_count, group_size, HEAD), segment_positions, segment_bias)
    ]
    start_states = tuple(
        [
            (
                jnp.full((grouped.shape[0], key_count, group_size), -jnp.inf, jnp.float32),
                jnp.zeros((grouped.shape[0], key_count, group_size), jnp.float32),
                jnp.zeros((grouped.shape[0], key_count, group_size, HEAD), jnp.float32),
            )
            for grouped, positions, bias in segments
        ]
    )
    piece_rows = lax.all_gather(
        keys_values.reshape(row_count, key_count, 2 * HEAD), "ep", axis=0, tiled=True
    )
    count_rows = piece_rows.shape[0]
    block_width = 512
    blocks = piece_rows.reshape(count_rows // block_width, block_width, key_count, 2 * HEAD)

    def one_block(states, scan_item):
        block_rows, block_index = scan_item
        first_key = block_index * block_width
        key_block = block_rows[:, :, :HEAD]
        value_block = block_rows[:, :, HEAD:]
        key_gate = lax.dynamic_slice_in_dim(forget_cache, first_key, block_width, 1).reshape(
            1, key_count, group_size, block_width
        )
        key_pos = first_key + jnp.arange(block_width, dtype=jnp.int32)
        updated = []
        for (grouped, positions, bias), state in zip(segments, states):

            def take_block(state_in, grouped=grouped, positions=positions, bias=bias):
                running_max, running_sum, weighted = state_in
                scores = (
                    jnp.einsum(
                        "qhgd,khd->qhgk", grouped, key_block, preferred_element_type=jnp.float32
                    )
                    * score_scale
                )
                scores = scores + bias - key_gate
                visible = (key_pos[None, :] <= positions[:, None])[:, None, None, :]
                scores = jnp.where(visible, scores, -jnp.inf)
                new_max = jnp.maximum(running_max, jnp.max(scores, axis=-1))
                safe_max = jnp.where(jnp.isfinite(new_max), new_max, 0.0)
                factor = jnp.exp(running_max - safe_max)
                weights = jnp.exp(scores - safe_max[..., None])
                running_sum = running_sum * factor + jnp.sum(weights, axis=-1)
                weighted = weighted * factor[..., None] + jnp.einsum(
                    "qhgk,khd->qhgd",
                    weights.astype(jnp.bfloat16),
                    value_block,
                    preferred_element_type=jnp.float32,
                )
                return (new_max, running_sum, weighted)

            def keep_state(state_in):
                return state_in

            updated.append(lax.cond(first_key <= positions[-1], take_block, keep_state, state))
        return (tuple(updated), None)

    final_states, _ = lax.scan(
        one_block, start_states, (blocks, jnp.arange(count_rows // block_width, dtype=jnp.int32))
    )
    outputs = [
        (weighted / running_sum[..., None])
        .reshape(running_sum.shape[0], query_count * HEAD)
        .astype(jnp.bfloat16)
        for running_max, running_sum, weighted in final_states
    ]
    attended = outputs[0]
    local_rows = lax.all_to_all(attended, "tp", split_axis=0, concat_axis=1, tiled=True)
    heads_normed = scaled_rows(local_rows, heads_gain)
    mixer_out = jnp.dot(heads_normed, output_weight, preferred_element_type=jnp.float32).astype(
        jnp.bfloat16
    )
    experts_count = lax.axis_size("ep")
    expert_rows, pick_count = routes.shape
    capacity = 2 * expert_rows * pick_count // experts_count
    expert_in = scaled_rows(expert_tokens, expert_gain)
    shifted = route_logits - jnp.max(route_logits, axis=1, keepdims=True)
    raised = jnp.exp(shifted)
    route_weight = raised / jnp.sum(raised, axis=1, keepdims=True)
    position, slot_token = assign_slots(routes, experts_count, capacity)
    model_width = expert_in.shape[1]
    part_width = model_width // lax.axis_size("tp")
    gate_local = gate_weight[0]
    up_local = up_weight[0]
    down_local = down_weight[0]
    own_columns = lax.dynamic_slice_in_dim(
        expert_in, lax.axis_index("tp") * part_width, part_width, 1
    )
    padded = jnp.concatenate([own_columns, jnp.zeros((1, part_width), jnp.bfloat16)], axis=0)
    outgoing = jnp.take(padded, slot_token, axis=0).reshape(experts_count, capacity, part_width)
    arrived = lax.all_to_all(outgoing, "ep", split_axis=0, concat_axis=0, tiled=True).reshape(
        experts_count * capacity, part_width
    )
    piece_rows = lax.all_gather(arrived, "tp", axis=1, tiled=True)
    gate_sum = jnp.dot(piece_rows, gate_local, preferred_element_type=jnp.float32)
    up_sum = jnp.dot(piece_rows, up_local, preferred_element_type=jnp.float32)
    gate_cut = jnp.minimum(gate_sum, clamp_limit)
    up_cut = jnp.clip(up_sum, -clamp_limit, clamp_limit)
    hidden = ((up_cut + 1.0) * gate_cut * jax.nn.sigmoid(sigmoid_slope * gate_cut)).astype(
        jnp.bfloat16
    )
    expert_out = lax.psum_scatter(
        lax.dot_general(
            down_local, hidden, (((0,), (1,)), ((), ())), preferred_element_type=jnp.float32
        ).astype(jnp.bfloat16),
        "tp",
        scatter_dimension=0,
        tiled=True,
    )
    returned = lax.all_to_all(expert_out, "ep", split_axis=1, concat_axis=1, tiled=True)
    picked = jnp.take(returned, position.reshape(-1), axis=1).reshape(
        part_width, expert_rows, pick_count
    )
    moe_out = jnp.einsum("crk,rk->rc", picked.astype(jnp.float32), route_weight).astype(
        jnp.bfloat16
    )
    return (mixer_out, moe_out)


MESH = pl.DeviceIdType.MESH


def fused_kernel(
    E, T, loads,
    q_ref, kv_ref, f_ref, hg_ref, ow_hbm, tok_ref, eg_ref, routes_ref, logits_ref,
    gw_hbm, uw_hbm, dw_hbm,
    mix_ref, moe_ref,
    ow, gw, uw, dw, tokall, kvall, qa, fa, m_sc, acc_sc,
    s1s, s1r, s1o, s2s, s2r, s3s, s3r, zs, zr, wtab, att, attall,
    wsem, ssem, tok_rs, kv_rs, s1_rs, s2_rs, s3_rs, z_rs, wt_rs, att_rs,
):
    f32, bf16 = jnp.float32, jnp.bfloat16
    e = lax.axis_index("ep")
    t = lax.axis_index("tp")
    B = 2
    A = E // B
    a, b = e // B, e % B
    y, c = t // 2, t % 2
    mate = y * 2 + (1 - c)
    across_y = (1 - y) * 2 + c
    across_x = a * B + (1 - b)
    rows = q_ref.shape[0]
    heads = q_ref.shape[1] // HEAD
    kv_heads = kv_ref.shape[1] // (2 * HEAD)
    group = heads // kv_heads
    erows, width = tok_ref.shape
    part = width // T
    lanes = 2 * HEAD

    weight_copies = [
        pltpu.make_async_copy(gw_hbm.at[0], gw, wsem.at[0]),
        pltpu.make_async_copy(uw_hbm.at[0], uw, wsem.at[1]),
        pltpu.make_async_copy(dw_hbm.at[0], dw, wsem.at[2]),
        pltpu.make_async_copy(ow_hbm, ow, wsem.at[3]),
    ]
    for copy in loads:
        copy.start()

    barrier = pltpu.get_barrier_semaphore()
    for d in range(1, E):
        pl.semaphore_signal(barrier, inc=1, device_id=(lax.rem(e + d, E), t), device_id_type=MESH)
    for d in range(1, T):
        pl.semaphore_signal(barrier, inc=1, device_id=(e, lax.rem(t + d, T)), device_id_type=MESH)

    for copy in loads:
        copy.wait()
    for copy in weight_copies:
        copy.start()

    tokens = tok_ref[...].astype(f32)
    inverse = lax.rsqrt(jnp.mean(tokens * tokens, axis=-1, keepdims=True) + epsilon)
    in_rows = (tokens * inverse * eg_ref[...]).astype(bf16)
    for quarter in range(T):
        tokall[quarter, e] = in_rows[:, quarter * part : (quarter + 1) * part]
    logits = logits_ref[...]
    raised = jnp.exp(logits - jnp.max(logits, axis=0, keepdims=True))
    weight = raised / jnp.sum(raised, axis=0, keepdims=True)
    chosen = routes_ref[...]
    wtab[e] = jnp.concatenate(
        [jnp.sum(jnp.where(chosen == j, weight, 0.0), axis=0, keepdims=True) for j in range(E)],
        axis=0,
    )
    with jax.named_scope("barrier"):
        pl.semaphore_wait(barrier, E - 1 + T - 1)

    sent = []

    def send(cond, src, dst, recv, device):
        slot = len(sent)

        def build():
            return pltpu.make_async_remote_copy(
                src_ref=src, dst_ref=dst, send_sem=ssem.at[slot], recv_sem=recv,
                device_id=device, device_id_type=MESH,
            )

        sent.append((cond, build))
        if cond is None:
            build().start()
        else:
            @pl.when(cond)
            def _():
                build().start()

    def arrive(cond, dst, recv):
        def go():
            pltpu.make_async_remote_copy(
                src_ref=dst, dst_ref=dst, send_sem=ssem.at[0], recv_sem=recv,
                device_id=(e, mate), device_id_type=MESH,
            ).wait_recv()

        if cond is None:
            go()
        else:
            pl.when(cond)(go)

    def both(p, q):
        return q if p is None else (p if q is None else jnp.logical_and(p, q))

    def send_token_block(cond, j, up, down, across, own=False):
        src = dst = tokall.at[t, j]
        recv = tok_rs.at[j, t]
        if up:
            send(both(cond, a + 1 < A), src, dst, recv, (e + B, t))
        if down:
            send(both(cond, a > 0), src, dst, recv, (e - B, t))
        if across:
            send(cond, src, dst, recv, (across_x, t))
        if not own:
            send(cond, src, dst, recv, (e, across_y))
            send(cond, src, dst, recv, (e, mate))

    def y_forward(cond, j):
        arrive(cond, tokall.at[across_y, j], tok_rs.at[j, across_y])
        send(cond, tokall.at[across_y, j], tokall.at[across_y, j], tok_rs.at[j, across_y], (e, mate))

    late = []

    def token_step(s):
        pending = list(late)
        late.clear()
        if s < A:
            up_ok, down_ok = a - s >= 0, a + s < A
            ju, jd = e - s * B, e + s * B
            arrive(up_ok, tokall.at[t, ju], tok_rs.at[ju, t])
            send_token_block(up_ok, ju, True, False, True)
            arrive(down_ok, tokall.at[t, jd], tok_rs.at[jd, t])
            send_token_block(down_ok, jd, False, True, True)
            late.extend([(up_ok, ju), (down_ok, jd)])
        if s <= A:
            for sign in (1, -1) if s > 1 else (1,):
                oa = a - sign * (s - 1)
                ok = None if s == 1 else (oa >= 0 if sign == 1 else oa < A)
                j = oa * B + (1 - b)
                arrive(ok, tokall.at[t, j], tok_rs.at[j, t])
                send_token_block(ok, j, False, False, False)
                late.append((ok, j))
        for cond, j in pending:
            y_forward(cond, j)

    def send_kv_block(cond, j):
        src = dst = kvall.at[j]
        recv = kv_rs.at[j]
        send(both(cond, a + 1 < A), src, dst, recv, (e + B, t))
        send(both(cond, across_x > j), src, dst, recv, (across_x, t))

    def kv_step(s):
        ok, j = a - s >= 0, e - s * B
        arrive(ok, kvall.at[j], kv_rs.at[j])
        send_kv_block(ok, j)

    def attend(j, diag):
        nc = rows // lanes
        tiles = list(range(heads))
        base = j * rows

        def score(h):
            lhs = jnp.concatenate(
                [kvall[j, :rows], fa[pl.ds(pl.multiple_of(base, rows), rows)]], axis=1
            )
            s = lax.dot_general(
                lhs, qa[h], (((1,), (1,)), ((), ())), preferred_element_type=f32
            )
            if diag:
                kp = lax.broadcasted_iota(jnp.int32, s.shape, 0)
                qp = lax.broadcasted_iota(jnp.int32, s.shape, 1)
                s = jnp.where(kp <= qp, s, -jnp.inf)
            return s

        def soften(h, s):
            top = jnp.max(s, axis=0, keepdims=True)
            factor = None
            if not diag:
                old = m_sc[h]
                top = jnp.maximum(top, old)
                factor = jnp.exp(old - top)
            m_sc[h] = top
            return jnp.exp(s - top).astype(bf16), factor

        def gather(h, p, factor):
            g = h // group
            vt = jnp.concatenate(
                [
                    kvall[j, rows + n * lanes + g * HEAD : rows + n * lanes + (g + 1) * HEAD]
                    for n in range(nc)
                ],
                axis=1,
            )
            lhs = jnp.concatenate([vt, jnp.ones((16, rows), bf16)], axis=0)
            pv = jnp.dot(lhs, p, preferred_element_type=f32)
            if not diag:
                pv = acc_sc[h] * factor + pv
            acc_sc[h] = pv

        held, soft = {}, {}
        for i in range(len(tiles) + 2):
            if i < len(tiles):
                held[i] = score(tiles[i])
            if 0 <= i - 1 < len(tiles):
                soft[i - 1] = soften(tiles[i - 1], held.pop(i - 1))
            if 0 <= i - 2 < len(tiles):
                gather(tiles[i - 2], *soft.pop(i - 2))

    def attend_if(cond, j, wait):
        @pl.when(cond)
        def _():
            if wait:
                arrive(None, kvall.at[j], kv_rs.at[j])
            with jax.named_scope("att"):
                attend(j, False)

    def up(s):
        attend_if(a - s >= 0, e - s * B, False)

    def side(s):
        j = (a - s) * B + (1 - b)
        attend_if(jnp.logical_and(a - s >= 0, j < e), j, True)

    crows = B * erows

    def chunk_z(i):
        if A == 4:
            half = a // 2
            return [a + 1 - 2 * (a % 2), 2 - half, 3 - 3 * half, a][i]
        return lax.rem(a + i + 1, A)

    def expert_chunk(i):
        start = chunk_z(i) * B
        mine = i == A - 1
        scale = []
        for k in range(B):
            for oy in range(2):
                quarter = oy * 2 + (1 - c)
                arrive(
                    (start + k != e) if mine else None,
                    tokall.at[quarter, start + k], tok_rs.at[start + k, quarter],
                )
            arrive((start + k != e) if mine else None, wtab.at[start + k], wt_rs.at[start + k])
            columns = wtab[start + k].T
            lane = lax.broadcasted_iota(jnp.int32, columns.shape, 1)
            scale.append(jnp.sum(jnp.where(lane == e, columns, 0.0), axis=1, keepdims=True))
        scale = jnp.concatenate(scale, axis=0)
        x = jnp.concatenate(
            [tokall[qt, pl.ds(start, B)].reshape(crows, part) for qt in range(T)], axis=1
        )
        gate = jnp.dot(x, gw[...], preferred_element_type=f32)
        up_sum = jnp.dot(x, uw[...], preferred_element_type=f32)
        gate = jnp.minimum(gate, clamp_limit)
        up_sum = jnp.clip(up_sum, -clamp_limit, clamp_limit)
        hidden = ((up_sum + 1.0) * gate * jax.nn.sigmoid(sigmoid_slope * gate)).astype(bf16)

        def down(oy, oc):
            col = pl.multiple_of((oy * 2 + oc) * part, part)
            out = jnp.dot(hidden, dw[:, pl.ds(col, part)], preferred_element_type=f32)
            return (out * scale).astype(bf16).reshape(B, erows, part)

        for p, oy in enumerate((1 - y, y)):
            s1s[i, p] = down(oy, 1 - c)
            send(None, s1s.at[i, p], s1r.at[i, p], s1_rs.at[i, p], (e, mate))
        for p, oy in enumerate((1 - y, y)):
            s1o[i, p] = down(oy, c)

    def add(*terms):
        total = terms[0].astype(f32)
        for term in terms[1:]:
            total = total + term.astype(f32)
        return total.astype(bf16)

    def pair_step(i):
        arrive(None, s1r.at[i, 0], s1_rs.at[i, 0])
        s2s[i] = add(s1o[i, 0], s1r[i, 0])
        send(None, s2s.at[i], s2r.at[i], s2_rs.at[i], (e, across_y))

    def y_step(i):
        arrive(None, s1r.at[i, 1], s1_rs.at[i, 1])
        arrive(None, s2r.at[i], s2_rs.at[i])
        s3s[i] = add(s1o[i, 1, 1 - b], s1r[i, 1, 1 - b], s2r[i, 1 - b])
        send(None, s3s.at[i], s3r.at[i], s3_rs.at[i], (across_x, t))

    def x_step(i):
        arrive(None, s3r.at[i], s3_rs.at[i])
        out = add(s1o[i, 1, b], s1r[i, 1, b], s2r[i, b], s3r[i])
        if i == A - 1:
            zr[a] = out
        else:
            zs[i] = out
            send(None, zs.at[i], zr.at[a], z_rs.at[a], (chunk_z(i) * B + b, t))

    def scoped(name, f, *args):
        with jax.named_scope(name):
            f(*args)

    send_token_block(None, e, True, True, True, own=True)
    for d in range(1, E):
        j = lax.rem(e + d, E)
        send(None, wtab.at[e], wtab.at[e], wt_rs.at[e], (j, t))

    def prepare():
        zero = jnp.zeros((rows, HEAD), bf16)
        lane = lax.broadcasted_iota(jnp.int32, (rows, lanes), 1)
        for h in range(heads):
            q = q_ref[:, h * HEAD : (h + 1) * HEAD] * jnp.asarray(0.125, bf16)
            qa[h, :, :lanes] = jnp.concatenate([q, zero] if h < group else [zero, q], axis=1)
            chosen_lane = (lane == h) | (lane == h + 8) | (lane == h + 16)
            qa[h, :, lanes:] = jnp.where(chosen_lane, -1.0, 0.0).astype(bf16)
        kvall[e, :rows] = jnp.concatenate(
            [kv_ref[:, g * lanes : g * lanes + HEAD] for g in range(kv_heads)], axis=1
        )
        values = jnp.concatenate(
            [kv_ref[:, g * lanes + HEAD : (g + 1) * lanes] for g in range(kv_heads)], axis=1
        )
        for n in range(rows // lanes):
            kvall[e, rows + n * lanes : rows + (n + 1) * lanes] = values[
                n * lanes : (n + 1) * lanes
            ].T
        first = f_ref[:, pl.ds(pl.multiple_of(e * rows, rows), lanes)][:, :1]
        gates = f_ref[...] - first
        high = gates.astype(bf16).astype(f32)
        rest = gates - high
        middle = rest.astype(bf16).astype(f32)
        low = rest - middle
        blank = jnp.zeros((8 - heads, gates.shape[1]), f32)
        stack = jnp.concatenate(
            [high, blank, middle, blank, low, blank, jnp.zeros((lanes - 24, gates.shape[1]), f32)],
            axis=0,
        )
        for n in range(gates.shape[1] // lanes):
            fa[n * lanes : (n + 1) * lanes] = stack[:, n * lanes : (n + 1) * lanes].T.astype(bf16)

    scoped("prepare", prepare)
    scoped("tok1", token_step, 1)
    scoped("tok2", token_step, 2)
    send_kv_block(None, e)
    scoped("diag", attend, e, True)
    scoped("tok3", token_step, 3)
    for copy in weight_copies[:3]:
        copy.wait()

    scoped("chunk0", expert_chunk, 0)
    scoped("tok4", token_step, 4)
    scoped("kv1", kv_step, 1)
    scoped("pair0", pair_step, 0)
    scoped("chunk1", expert_chunk, 1)
    scoped("tok5", token_step, 5)
    scoped("pair1", pair_step, 1)
    up(1)
    scoped("y0", y_step, 0)
    scoped("chunk2", expert_chunk, 2)
    scoped("kv2", kv_step, 2)
    scoped("pair2", pair_step, 2)
    side(0)
    scoped("y1", y_step, 1)
    scoped("x0", x_step, 0)
    scoped("chunk3", expert_chunk, 3)
    scoped("pair3", pair_step, 3)
    up(2)
    side(1)
    scoped("kv3", kv_step, 3)
    scoped("y2", y_step, 2)
    scoped("x1", x_step, 1)
    up(3)
    side(2)
    scoped("y3", y_step, 3)
    scoped("x2", x_step, 2)
    side(3)

    def attention_out():
        arows = rows // T
        for h in range(heads):
            acc = acc_sc[h]
            out = (acc[:HEAD] / acc[HEAD : HEAD + 1]).T.astype(bf16)
            for tt in range(T):
                att[tt, :, h * HEAD : (h + 1) * HEAD] = out[tt * arows : (tt + 1) * arows]
        attall[t] = att[t]
        for d in range(1, T):
            ot = lax.rem(t + d, T)
            send(None, att.at[ot], attall.at[t], att_rs.at[t], (e, ot))

    scoped("attout", attention_out)
    scoped("x3", x_step, 3)
    weight_copies[3].wait()

    def mixer():
        for d in range(1, T):
            ot = lax.rem(t + d, T)
            arrive(None, attall.at[ot], att_rs.at[ot])
        mixed = jnp.concatenate([attall[tt] for tt in range(T)], axis=1).astype(f32)
        inverse = lax.rsqrt(jnp.mean(mixed * mixed, axis=-1, keepdims=True) + epsilon)
        mixed = (mixed * inverse * hg_ref[...]).astype(bf16)
        mix_ref[...] = jnp.dot(mixed, ow[...], preferred_element_type=f32).astype(bf16)

    scoped("mixer", mixer)

    def combine():
        for d in range(1, A):
            oz = lax.rem(a + d, A)
            arrive(None, zr.at[oz], z_rs.at[oz])
        moe_ref[...] = add(*[zr[oz] for oz in range(A)])

    scoped("combine", combine)

    for cond, build in sent:
        if cond is None:
            build().wait_send()
        else:
            @pl.when(cond)
            def _():
                build().wait_send()


def fused_body(*args):
    (queries, keys_values, forget_cache, heads_gain, output_weight, expert_tokens,
     expert_gain, routes, route_logits, gate_weight, up_weight, down_weight) = args
    E, T = lax.axis_size("ep"), lax.axis_size("tp")
    rows = queries.shape[0]
    heads = queries.shape[1] // HEAD
    erows, width = expert_tokens.shape
    part = width // T
    B = 2
    A = E // B
    bf16, f32 = jnp.bfloat16, jnp.float32
    V, DMA = pltpu.VMEM, pltpu.SemaphoreType.DMA
    vm = pl.BlockSpec(memory_space=pltpu.VMEM)
    hbm = pl.BlockSpec(memory_space=pltpu.HBM)

    operands = [
        queries, keys_values, forget_cache, heads_gain.reshape(1, -1), output_weight, expert_tokens,
        expert_gain.reshape(1, -1), routes.T, route_logits.T, gate_weight, up_weight, down_weight,
    ]
    small = [5, 6, 7, 8, 1, 0, 2, 3]

    def kernel(*refs):
        refs = list(refs)
        load_sem = refs.pop()
        held = refs[-len(small) :]
        refs = refs[: -len(small)]
        loads = []
        for n, (index, place) in enumerate(zip(small, held)):
            loads.append(pltpu.make_async_copy(refs[index], place, load_sem.at[n]))
            refs[index] = place
        fused_kernel(E, T, loads, *refs)

    return pl.pallas_call(
        kernel,
        out_shape=(
            jax.ShapeDtypeStruct((rows // T, output_weight.shape[1]), bf16),
            jax.ShapeDtypeStruct((erows, part), bf16),
        ),
        in_specs=[hbm] * len(operands),
        out_specs=(vm, vm),
        scratch_shapes=[
            V(output_weight.shape, bf16),
            V(gate_weight.shape[1:], bf16),
            V(up_weight.shape[1:], bf16),
            V(down_weight.shape[1:], bf16),
            V((T, E, erows, part), bf16),
            V((E, 2 * rows, 2 * HEAD), bf16),
            V((heads, rows, 4 * HEAD), bf16),
            V((E * rows, 2 * HEAD), bf16),
            V((heads, 1, rows), f32),
            V((heads, HEAD + 16, rows), f32),
            V((A, 2, B, erows, part), bf16),
            V((A, 2, B, erows, part), bf16),
            V((A, 2, B, erows, part), bf16),
            V((A, B, erows, part), bf16),
            V((A, B, erows, part), bf16),
            V((A, erows, part), bf16),
            V((A, erows, part), bf16),
            V((A, erows, part), bf16),
            V((A, erows, part), bf16),
            V((E, E, erows), f32),
            V((T, rows // T, queries.shape[1]), bf16),
            V((T, rows // T, queries.shape[1]), bf16),
            DMA((4,)),
            DMA((128,)),
            DMA((E, T)),
            DMA((E,)),
            DMA((A, 2)),
            DMA((A,)),
            DMA((A,)),
            DMA((A,)),
            DMA((E,)),
            DMA((T,)),
        ]
        + [V(operands[n].shape, operands[n].dtype) for n in small]
        + [DMA((len(small),))],
        compiler_params=pltpu.CompilerParams(
            collective_id=0, has_side_effects=True, vmem_limit_bytes=60 * 1024 * 1024
        ),
    )(*operands)


def pick_body(*args):
    queries, keys_values, routes = args[0], args[1], args[7]
    rows, picks = routes.shape
    E, T = lax.axis_size("ep"), lax.axis_size("tp")
    capacity = 2 * rows * picks // E
    shapes = queries.shape[1] == 4 * HEAD and keys_values.shape[1] == 4 * HEAD
    if capacity >= rows and T == 4 and E == 8 and shapes:
        return fused_body(*args)
    return body(*args)


def solution(mesh):
    placed = (
        P("ep", "tp"),
        P("ep", "tp"),
        P("tp", None),
        P(),
        P(),
        P("ep", None),
        P(),
        P("ep", None),
        P("ep", None),
        P("ep", None, "tp"),
        P("ep", None, "tp"),
        P("ep", "tp", None),
    )
    return jax.shard_map(
        pick_body,
        mesh=mesh,
        in_specs=placed,
        out_specs=(P(("ep", "tp"), None), P("ep", "tp")),
        check_vma=False,
    )
```

```python
import math

import jax
import jax.numpy as jnp
from jax import lax
from jax.experimental import pallas as pl
from jax.experimental.pallas import tpu as pltpu
from jax.sharding import PartitionSpec as P

HEAD = 64


epsilon = 1e-06
clamp_limit = 7.0
sigmoid_slope = 1.702


def scaled_rows(values, gain_vector):
    as_float = values.astype(jnp.float32)
    inverse = lax.rsqrt(jnp.mean(as_float * as_float, axis=-1, keepdims=True) + epsilon)
    return (as_float * inverse * gain_vector).astype(jnp.bfloat16)


def assign_slots(routes, experts, capacity):
    row_count, pick_count = routes.shape
    flat_routes = routes.reshape(-1)
    onehot = (flat_routes[:, None] == jnp.arange(experts, dtype=jnp.int32)[None, :]).astype(
        jnp.int32
    )
    earlier = jnp.cumsum(onehot, axis=0) - onehot
    slot_rank = jnp.sum(earlier * onehot, axis=1)
    position = flat_routes * capacity + slot_rank
    owner_row = jnp.arange(row_count * pick_count, dtype=jnp.int32) // pick_count
    slot_token = jnp.full((experts * capacity,), row_count, jnp.int32).at[position].set(owner_row)
    return (position.reshape(row_count, pick_count), slot_token)


def body(
    queries,
    keys_values,
    forget_cache,
    heads_gain,
    output_weight,
    expert_tokens,
    expert_gain,
    routes,
    route_logits,
    gate_weight,
    up_weight,
    down_weight,
):
    row_count = queries.shape[0]
    query_count = queries.shape[1] // HEAD
    key_count = keys_values.shape[1] // (2 * HEAD)
    group_size = query_count // key_count
    offset = lax.axis_index("ep") * row_count
    score_scale = 1.0 / math.sqrt(HEAD)
    count_rows = queries.shape[0]
    segment_positions = offset + jnp.arange(count_rows, dtype=jnp.int32)
    gate_rows = lax.dynamic_slice_in_dim(forget_cache, offset, count_rows, 1)
    segment_bias = gate_rows.T.reshape(count_rows, key_count, group_size, 1)
    segments = [
        (queries.reshape(count_rows, key_count, group_size, HEAD), segment_positions, segment_bias)
    ]
    start_states = tuple(
        [
            (
                jnp.full((grouped.shape[0], key_count, group_size), -jnp.inf, jnp.float32),
                jnp.zeros((grouped.shape[0], key_count, group_size), jnp.float32),
                jnp.zeros((grouped.shape[0], key_count, group_size, HEAD), jnp.float32),
            )
            for grouped, positions, bias in segments
        ]
    )
    piece_rows = lax.all_gather(
        keys_values.reshape(row_count, key_count, 2 * HEAD), "ep", axis=0, tiled=True
    )
    count_rows = piece_rows.shape[0]
    block_width = 512
    blocks = piece_rows.reshape(count_rows // block_width, block_width, key_count, 2 * HEAD)

    def one_block(states, scan_item):
        block_rows, block_index = scan_item
        first_key = block_index * block_width
        key_block = block_rows[:, :, :HEAD]
        value_block = block_rows[:, :, HEAD:]
        key_gate = lax.dynamic_slice_in_dim(forget_cache, first_key, block_width, 1).reshape(
            1, key_count, group_size, block_width
        )
        key_pos = first_key + jnp.arange(block_width, dtype=jnp.int32)
        updated = []
        for (grouped, positions, bias), state in zip(segments, states):

            def take_block(state_in, grouped=grouped, positions=positions, bias=bias):
                running_max, running_sum, weighted = state_in
                scores = (
                    jnp.einsum(
                        "qhgd,khd->qhgk", grouped, key_block, preferred_element_type=jnp.float32
                    )
                    * score_scale
                )
                scores = scores + bias - key_gate
                visible = (key_pos[None, :] <= positions[:, None])[:, None, None, :]
                scores = jnp.where(visible, scores, -jnp.inf)
                new_max = jnp.maximum(running_max, jnp.max(scores, axis=-1))
                safe_max = jnp.where(jnp.isfinite(new_max), new_max, 0.0)
                factor = jnp.exp(running_max - safe_max)
                weights = jnp.exp(scores - safe_max[..., None])
                running_sum = running_sum * factor + jnp.sum(weights, axis=-1)
                weighted = weighted * factor[..., None] + jnp.einsum(
                    "qhgk,khd->qhgd",
                    weights.astype(jnp.bfloat16),
                    value_block,
                    preferred_element_type=jnp.float32,
                )
                return (new_max, running_sum, weighted)

            def keep_state(state_in):
                return state_in

            updated.append(lax.cond(first_key <= positions[-1], take_block, keep_state, state))
        return (tuple(updated), None)

    final_states, _ = lax.scan(
        one_block, start_states, (blocks, jnp.arange(count_rows // block_width, dtype=jnp.int32))
    )
    outputs = [
        (weighted / running_sum[..., None])
        .reshape(running_sum.shape[0], query_count * HEAD)
        .astype(jnp.bfloat16)
        for running_max, running_sum, weighted in final_states
    ]
    attended = outputs[0]
    local_rows = lax.all_to_all(attended, "tp", split_axis=0, concat_axis=1, tiled=True)
    heads_normed = scaled_rows(local_rows, heads_gain)
    mixer_out = jnp.dot(heads_normed, output_weight, preferred_element_type=jnp.float32).astype(
        jnp.bfloat16
    )
    experts_count = lax.axis_size("ep")
    expert_rows, pick_count = routes.shape
    capacity = 2 * expert_rows * pick_count // experts_count
    expert_in = scaled_rows(expert_tokens, expert_gain)
    shifted = route_logits - jnp.max(route_logits, axis=1, keepdims=True)
    raised = jnp.exp(shifted)
    route_weight = raised / jnp.sum(raised, axis=1, keepdims=True)
    position, slot_token = assign_slots(routes, experts_count, capacity)
    model_width = expert_in.shape[1]
    part_width = model_width // lax.axis_size("tp")
    gate_local = gate_weight[0]
    up_local = up_weight[0]
    down_local = down_weight[0]
    own_columns = lax.dynamic_slice_in_dim(
        expert_in, lax.axis_index("tp") * part_width, part_width, 1
    )
    padded = jnp.concatenate([own_columns, jnp.zeros((1, part_width), jnp.bfloat16)], axis=0)
    outgoing = jnp.take(padded, slot_token, axis=0).reshape(experts_count, capacity, part_width)
    arrived = lax.all_to_all(outgoing, "ep", split_axis=0, concat_axis=0, tiled=True).reshape(
        experts_count * capacity, part_width
    )
    piece_rows = lax.all_gather(arrived, "tp", axis=1, tiled=True)
    gate_sum = jnp.dot(piece_rows, gate_local, preferred_element_type=jnp.float32)
    up_sum = jnp.dot(piece_rows, up_local, preferred_element_type=jnp.float32)
    gate_cut = jnp.minimum(gate_sum, clamp_limit)
    up_cut = jnp.clip(up_sum, -clamp_limit, clamp_limit)
    hidden = ((up_cut + 1.0) * gate_cut * jax.nn.sigmoid(sigmoid_slope * gate_cut)).astype(
        jnp.bfloat16
    )
    expert_out = lax.psum_scatter(
        lax.dot_general(
            down_local, hidden, (((0,), (1,)), ((), ())), preferred_element_type=jnp.float32
        ).astype(jnp.bfloat16),
        "tp",
        scatter_dimension=0,
        tiled=True,
    )
    returned = lax.all_to_all(expert_out, "ep", split_axis=1, concat_axis=1, tiled=True)
    picked = jnp.take(returned, position.reshape(-1), axis=1).reshape(
        part_width, expert_rows, pick_count
    )
    moe_out = jnp.einsum("crk,rk->rc", picked.astype(jnp.float32), route_weight).astype(
        jnp.bfloat16
    )
    return (mixer_out, moe_out)


MESH = pl.DeviceIdType.MESH
SEND_SLOTS = 96


def fused_kernel(
    E, T, loads,
    q_ref, kv_ref, f_ref, hg_ref, ow_hbm, tok_ref, eg_ref, routes_ref, logits_ref,
    gw_hbm, uw_hbm, dw_hbm,
    mix_ref, moe_ref,
    ow, gw, uw, dw, tokall, qraw, kvraw, qx, kvx, kvall, qa, fa, m_sc, acc_sc,
    s1s, s1r, s1o, s2s, s2r, s3s, s3r, zs, zr, wtab, att, attall,
    wsem, ssem, tok_rs, top_rs, qx_rs, kvx_rs, kv_rs, s1_rs, s2_rs, s3_rs, z_rs, wt_rs,
    att_rs,
):
    f32, bf16 = jnp.float32, jnp.bfloat16
    e = lax.axis_index("ep")
    t = lax.axis_index("tp")
    B = 2
    A = E // B
    a, b = e // B, e % B
    y, c = t // 2, t % 2
    mate = y * 2 + (1 - c)
    across_y = (1 - y) * 2 + c
    across_x = a * B + (1 - b)
    rows = q_ref.shape[0]
    heads = q_ref.shape[1] // HEAD // B
    erows, width = tok_ref.shape
    part = width // T
    half = part // 2
    lanes = 2 * HEAD
    extra = erows // 4
    loads = loads + [
        pltpu.make_async_copy(ref.at[:, g * lanes : (g + 1) * lanes], place.at[g], wsem.at[4 + 2 * n + g])
        for n, (ref, place) in enumerate(((kv_ref, kvraw), (q_ref, qraw)))
        for g in range(B)
    ]

    weight_copies = [
        pltpu.make_async_copy(gw_hbm.at[0], gw, wsem.at[0]),
        pltpu.make_async_copy(uw_hbm.at[0], uw, wsem.at[1]),
        pltpu.make_async_copy(dw_hbm.at[0], dw, wsem.at[2]),
        pltpu.make_async_copy(ow_hbm, ow, wsem.at[3]),
    ]
    for copy in loads:
        copy.start()

    barrier = pltpu.get_barrier_semaphore()
    for d in range(1, E):
        pl.semaphore_signal(barrier, inc=1, device_id=(lax.rem(e + d, E), t), device_id_type=MESH)
    for d in range(1, T):
        ot = lax.rem(t + d, T)
        pl.semaphore_signal(barrier, inc=1, device_id=(e, ot), device_id_type=MESH)
        pl.semaphore_signal(barrier, inc=1, device_id=(across_x, ot), device_id_type=MESH)

    for copy in loads:
        copy.wait()
    for copy in weight_copies:
        copy.start()

    tokens = tok_ref[...].astype(f32)
    inverse = lax.rsqrt(jnp.mean(tokens * tokens, axis=-1, keepdims=True) + epsilon)
    in_rows = (tokens * inverse * eg_ref[...]).astype(bf16)
    for quarter in range(T):
        tokall[quarter, e] = in_rows[:, quarter * part : (quarter + 1) * part]
    logits = logits_ref[...]
    raised = jnp.exp(logits - jnp.max(logits, axis=0, keepdims=True))
    weight = raised / jnp.sum(raised, axis=0, keepdims=True)
    chosen = routes_ref[...]
    wtab[e] = jnp.concatenate(
        [jnp.sum(jnp.where(chosen == j, weight, 0.0), axis=0, keepdims=True) for j in range(E)],
        axis=0,
    )
    with jax.named_scope("barrier"):
        pl.semaphore_wait(barrier, E - 1 + 2 * (T - 1))

    sent, free = [], list(range(SEND_SLOTS))

    def send(cond, src, dst, recv, device):
        slot = free.pop(0)

        def build():
            return pltpu.make_async_remote_copy(
                src_ref=src, dst_ref=dst, send_sem=ssem.at[slot], recv_sem=recv,
                device_id=device, device_id_type=MESH,
            )

        sent.append((slot, cond, build))
        if cond is None:
            build().start()
        else:
            @pl.when(cond)
            def _():
                build().start()

    def retire(entries):
        for entry in list(entries):
            slot, cond, build = entry
            if cond is None:
                build().wait_send()
            else:
                @pl.when(cond)
                def _():
                    build().wait_send()
            sent.remove(entry)
            free.append(slot)

    def arrive(cond, dst, recv):
        def go():
            pltpu.make_async_remote_copy(
                src_ref=dst, dst_ref=dst, send_sem=ssem.at[0], recv_sem=recv,
                device_id=(e, mate), device_id_type=MESH,
            ).wait_recv()

        if cond is None:
            go()
        else:
            pl.when(cond)(go)

    def both(p, q):
        return q if p is None else (p if q is None else jnp.logical_and(p, q))

    def send_token_block(cond, j, up, down, across, own=False):
        pieces = [(tokall.at[t, j], tok_rs.at[j, t])]
        if not (up is False and down is False and across is False):
            pieces.append((tokall.at[across_y, j, :extra], top_rs.at[j]))
        for ref, recv in pieces:
            for go, inside, to in (
                (up, a + 1 < A, (e + B, t)),
                (down, a > 0, (e - B, t)),
                (across, None, (across_x, t)),
            ):
                if go is not False:
                    send(both(cond, both(None if go is True else go, inside)), ref, ref, recv, to)
        if not own:
            ref = tokall.at[t, j, extra:]
            send(cond, ref, ref, tok_rs.at[j, t], (e, across_y))
            ref = tokall.at[t, j]
            send(cond, ref, ref, tok_rs.at[j, t], (e, mate))

    def arrive_token(cond, j):
        arrive(cond, tokall.at[t, j], tok_rs.at[j, t])
        arrive(cond, tokall.at[across_y, j, :extra], top_rs.at[j])

    def y_forward(cond, j):
        arrive(cond, tokall.at[across_y, j, extra:], tok_rs.at[j, across_y])
        ref = tokall.at[across_y, j]
        send(cond, ref, ref, tok_rs.at[j, across_y], (e, mate))

    late = []

    def token_step(s):
        pending = list(late)
        late.clear()
        if s < A:
            up_ok, down_ok = a - s >= 0, a + s < A
            ju, jd = e - s * B, e + s * B
            arrive_token(up_ok, ju)
            send_token_block(up_ok, ju, True, False, a - s > 0)
            arrive_token(down_ok, jd)
            send_token_block(down_ok, jd, False, True, a + s < A - 1)
            late.extend([(up_ok, ju), (down_ok, jd)])
        if s <= A:
            for sign in (1, -1) if s > 1 else (0,):
                oa = a - sign * (s - 1)
                ok = None if s == 1 else (oa >= 0 if sign == 1 else oa < A)
                j = oa * B + (1 - b)
                arrive_token(ok, j)
                rise = oa == 0 if sign >= 0 else False
                fall = oa == A - 1 if sign <= 0 else False
                send_token_block(ok, j, rise, fall, False)
                late.append((ok, j))
        for cond, j in pending:
            y_forward(cond, j)

    def swap_kv():
        send(None, kvraw.at[1 - b], kvx, kvx_rs.at[0], (across_x, t))

    def swap_q():
        send(None, qraw.at[1 - b], qx, qx_rs.at[0], (across_x, t))

    def send_kv_row(cond, row):
        send(both(cond, a + 1 < A), kvall.at[row], kvall.at[row], kv_rs.at[row], (e + B, t))

    def kv_step(s):
        ok, row = a - s >= 0, a - s
        arrive(ok, kvall.at[row], kv_rs.at[row])
        send_kv_row(ok, row)

    def by_block(mine, other):
        return [jnp.where(b == 0, mine, other), jnp.where(b == 0, other, mine)]

    def pack_kv():
        arrive(None, kvx, kvx_rs.at[0])
        blocks = by_block(kvraw[b], kvx[...])
        kvall[a, :rows] = jnp.concatenate([block[:, :HEAD] for block in blocks], axis=1)
        values = jnp.concatenate([block[:, HEAD:] for block in blocks], axis=1)
        for n in range(rows // lanes):
            kvall[a, rows + n * lanes : rows + (n + 1) * lanes] = values[
                n * lanes : (n + 1) * lanes
            ].T
        send_kv_row(None, a)

    def pack_q():
        arrive(None, qx, qx_rs.at[0])
        zero = jnp.zeros((rows, HEAD), bf16)
        lane = lax.broadcasted_iota(jnp.int32, (rows, lanes), 1)
        for xb, block in enumerate(by_block(qraw[b], qx[...])):
            block = block * jnp.asarray(0.125, bf16)
            for h in range(heads):
                q = block[:, h * HEAD : (h + 1) * HEAD]
                chosen_lane = (lane == h) | (lane == h + 8) | (lane == h + 16)
                pick = jnp.where(chosen_lane, -1.0, 0.0).astype(bf16)
                for kb in range(B):
                    qa[h, xb, kb, :, :lanes] = jnp.concatenate(
                        [q, zero] if kb == 0 else [zero, q], axis=1
                    )
                    qa[h, xb, kb, :, lanes:] = pick

    def pack_gates():
        count = f_ref.shape[1]
        gates = f_ref[...]
        gates = jnp.where(b == 0, gates[:heads], gates[heads:])
        first = f_ref[:, pl.ds(pl.multiple_of(a * B * rows, rows), lanes)][:, :1]
        gates = gates - jnp.where(b == 0, first[:heads], first[heads:])
        high = gates.astype(bf16).astype(f32)
        rest = gates - high
        middle = rest.astype(bf16).astype(f32)
        low = rest - middle
        blank = jnp.zeros((8 - heads, count), f32)
        stack = jnp.concatenate(
            [high, blank, middle, blank, low, blank, jnp.zeros((lanes - 24, count), f32)], axis=0
        )
        for n in range(count // lanes):
            fa[n * lanes : (n + 1) * lanes] = stack[:, n * lanes : (n + 1) * lanes].T.astype(bf16)

    def attend(row, tiles):
        nc = rows // lanes

        def score(h, xb, kb, start):
            gate = fa[pl.ds(pl.multiple_of((row * B + kb) * rows, rows), rows)]
            lhs = jnp.concatenate([kvall[row, :rows], gate], axis=1)
            s = lax.dot_general(
                lhs, qa[h, xb, kb], (((1,), (1,)), ((), ())), preferred_element_type=f32
            )
            if start is not None and xb == kb:
                kp = lax.broadcasted_iota(jnp.int32, s.shape, 0)
                qp = lax.broadcasted_iota(jnp.int32, s.shape, 1)
                s = jnp.where(kp <= qp, s, -jnp.inf)
            return s

        def soften(h, xb, kb, start, s):
            top = jnp.max(s, axis=0, keepdims=True)
            factor = None
            if not start:
                old = m_sc[h, xb]
                top = jnp.maximum(top, old)
                factor = jnp.exp(old - top)
            m_sc[h, xb] = top
            return jnp.exp(s - top).astype(bf16), factor

        def gather(h, xb, kb, start, p, factor):
            vt = jnp.concatenate(
                [
                    kvall[row, rows + n * lanes + kb * HEAD : rows + n * lanes + (kb + 1) * HEAD]
                    for n in range(nc)
                ],
                axis=1,
            )
            lhs = jnp.concatenate([vt, jnp.ones((16, rows), bf16)], axis=0)
            pv = jnp.dot(lhs, p, preferred_element_type=f32)
            if not start:
                pv = acc_sc[h, xb] * factor + pv
            acc_sc[h, xb] = pv

        held, soft = {}, {}
        for i in range(len(tiles) + 2):
            if i < len(tiles):
                held[i] = score(*tiles[i])
            if 0 <= i - 1 < len(tiles):
                soft[i - 1] = soften(*tiles[i - 1], held.pop(i - 1))
            if 0 <= i - 2 < len(tiles):
                gather(*tiles[i - 2], *soft.pop(i - 2))

    def attend_own():
        tiles = [(h, xb, xb, True) for xb in range(B) for h in range(heads)]
        tiles += [(h, xb, kb, False) for xb in range(B) for kb in range(xb) for h in range(heads)]
        own = [(h, xb, kb, start) for h, xb, kb, start in tiles]
        attend(a, own)

    def up(s, xb):
        @pl.when(a - s >= 0)
        def _():
            with jax.named_scope("att"):
                attend(a - s, [(h, xb, kb, None) for kb in range(B) for h in range(heads)])

    crows = B * erows

    def chunk_z(i):
        if A == 4:
            return [a + 1 - 2 * (a % 2), 2 - a // 2, 3 - 3 * (a // 2), a][i]
        return lax.rem(a + i + 1, A)

    def expert_chunk(i):
        start = chunk_z(i) * B
        mine = i == A - 1
        scale = []
        for k in range(B):
            for oy in range(2):
                quarter = oy * 2 + (1 - c)
                arrive(
                    (start + k != e) if mine else None,
                    tokall.at[quarter, start + k], tok_rs.at[start + k, quarter],
                )
            arrive((start + k != e) if mine else None, wtab.at[start + k], wt_rs.at[start + k])
            columns = wtab[start + k].T
            lane = lax.broadcasted_iota(jnp.int32, columns.shape, 1)
            scale.append(jnp.sum(jnp.where(lane == e, columns, 0.0), axis=1, keepdims=True))
        scale = jnp.concatenate(scale, axis=0)
        x = jnp.concatenate(
            [tokall[qt, pl.ds(start, B)].reshape(crows, part) for qt in range(T)], axis=1
        )
        gate = jnp.dot(x, gw[...], preferred_element_type=f32)
        up_sum = jnp.dot(x, uw[...], preferred_element_type=f32)
        gate = jnp.minimum(gate, clamp_limit)
        up_sum = jnp.clip(up_sum, -clamp_limit, clamp_limit)
        hidden = ((up_sum + 1.0) * gate * jax.nn.sigmoid(sigmoid_slope * gate)).astype(bf16)

        def down(oy, oc, place):
            col = pl.multiple_of((oy * 2 + oc) * part, part)
            out = jnp.dot(hidden, dw[:, pl.ds(col, part)], preferred_element_type=f32)
            out = (out * scale).astype(bf16)
            for n in range(2):
                place[n] = out[:, n * half : (n + 1) * half].reshape(B, erows, half)

        for p, oy in enumerate((1 - y, y)):
            down(oy, 1 - c, s1s.at[i, :, p])
        for n in range(2):
            send(None, s1s.at[i, n], s1r.at[i, n], s1_rs.at[i, n], (e, mate))
        for p, oy in enumerate((1 - y, y)):
            down(oy, c, s1o.at[i, :, p])

    def add(*terms):
        total = terms[0].astype(f32)
        for term in terms[1:]:
            total = total + term.astype(f32)
        return total.astype(bf16)

    def first_step(i):
        arrive(None, s1r.at[i, 0], s1_rs.at[i, 0])
        s2s[i, 0] = add(s1o[i, 0, 0], s1r[i, 0, 0])
        send(None, s2s.at[i, 0], s2r.at[i, 0], s2_rs.at[i, 0], (e, across_y))
        arrive(None, s1r.at[i, 1], s1_rs.at[i, 1])
        for p in range(2):
            s2s[i, 1, p] = add(s1o[i, 1, p, 1 - b], s1r[i, 1, p, 1 - b])
        send(None, s2s.at[i, 1], s2r.at[i, 1], s2_rs.at[i, 1], (across_x, t))

    def second_step(i):
        arrive(None, s2r.at[i, 0], s2_rs.at[i, 0])
        s3s[i, 0] = add(s1o[i, 0, 1, 1 - b], s1r[i, 0, 1, 1 - b], s2r[i, 0, 1 - b])
        send(None, s3s.at[i, 0], s3r.at[i, 0], s3_rs.at[i, 0], (across_x, t))
        arrive(None, s2r.at[i, 1], s2_rs.at[i, 1])
        s3s[i, 1] = add(s1o[i, 1, 0, b], s1r[i, 1, 0, b], s2r[i, 1, 0])
        send(None, s3s.at[i, 1], s3r.at[i, 1], s3_rs.at[i, 1], (e, across_y))

    def third_step(i):
        place = zr.at[a] if i == A - 1 else zs.at[i]
        arrive(None, s3r.at[i, 0], s3_rs.at[i, 0])
        place[0] = add(s1o[i, 0, 1, b], s1r[i, 0, 1, b], s2r[i, 0, b], s3r[i, 0])
        arrive(None, s3r.at[i, 1], s3_rs.at[i, 1])
        place[1] = add(s1o[i, 1, 1, b], s1r[i, 1, 1, b], s2r[i, 1, 1], s3r[i, 1])
        if i != A - 1:
            send(None, zs.at[i], zr.at[a], z_rs.at[a], (chunk_z(i) * B + b, t))

    def scoped(name, f, *args):
        with jax.named_scope(name):
            f(*args)

    send_token_block(None, e, True, True, True, own=True)
    for d in range(1, E):
        j = lax.rem(e + d, E)
        send(None, wtab.at[e], wtab.at[e], wt_rs.at[e], (j, t))

    swap_kv()
    scoped("gates", pack_gates)
    scoped("tok1", token_step, 1)
    swap_q()
    scoped("tok2", token_step, 2)
    scoped("packkv", pack_kv)
    scoped("packq", pack_q)
    scoped("own", attend_own)
    scoped("tok3", token_step, 3)
    for copy in weight_copies[:3]:
        copy.wait()
    retire(sent[:33])
    scoped("chunk0", expert_chunk, 0)
    scoped("tok4", token_step, 4)
    scoped("kv1", kv_step, 1)
    up(1, 0)
    scoped("r1_0", first_step, 0)
    scoped("tok5", token_step, 5)
    scoped("chunk1", expert_chunk, 1)
    up(1, 1)
    scoped("r1_1", first_step, 1)
    retire(sent[:44])
    scoped("kv2", kv_step, 2)
    scoped("r2_0", second_step, 0)
    scoped("chunk2", expert_chunk, 2)
    up(2, 0)
    scoped("r1_2", first_step, 2)
    scoped("r2_1", second_step, 1)
    scoped("r3_0", third_step, 0)
    scoped("chunk3", expert_chunk, 3)
    scoped("kv3", kv_step, 3)
    up(2, 1)
    scoped("r1_3", first_step, 3)
    scoped("r2_2", second_step, 2)
    scoped("r3_1", third_step, 1)

    arows = rows // T

    def attention_out(xb):
        out = jnp.concatenate(
            [acc_sc[h, xb, :HEAD] / acc_sc[h, xb, HEAD : HEAD + 1] for h in range(heads)], axis=0
        ).T.astype(bf16)
        for tt in range(T):
            att[xb, tt] = out[tt * arows : (tt + 1) * arows]

        @pl.when(b == xb)
        def _():
            attall[t, b] = att[xb, t]

        for d in range(T):
            ot = lax.rem(t + d, T)
            send(
                None if d else b != xb,
                att.at[xb, ot], attall.at[t, b], att_rs.at[t, b], (a * B + xb, ot),
            )

    up(3, 0)
    scoped("attout0", attention_out, 0)
    up(3, 1)
    scoped("attout1", attention_out, 1)
    scoped("r2_3", second_step, 3)
    scoped("r3_2", third_step, 2)
    scoped("r3_3", third_step, 3)
    weight_copies[3].wait()

    def mixer():
        for dx in range(B):
            for d in range(T):
                if dx or d:
                    ob, ot = lax.rem(b + dx, B), lax.rem(t + d, T)
                    arrive(None, attall.at[ot, ob], att_rs.at[ot, ob])
        mixed = jnp.concatenate(
            [attall[tt, bb] for tt in range(T) for bb in range(B)], axis=1
        ).astype(f32)
        inverse = lax.rsqrt(jnp.mean(mixed * mixed, axis=-1, keepdims=True) + epsilon)
        mixed = (mixed * inverse * hg_ref[...]).astype(bf16)
        mix_ref[...] = jnp.dot(mixed, ow[...], preferred_element_type=f32).astype(bf16)

    scoped("mixer", mixer)

    def combine():
        for d in range(1, A):
            oz = lax.rem(a + d, A)
            arrive(None, zr.at[oz], z_rs.at[oz])
        for n in range(2):
            moe_ref[:, n * half : (n + 1) * half] = add(*[zr[oz, n] for oz in range(A)])

    scoped("combine", combine)

    with jax.named_scope("drain"):
        retire(sent)


def fused_body(*args):
    (queries, keys_values, forget_cache, heads_gain, output_weight, expert_tokens,
     expert_gain, routes, route_logits, gate_weight, up_weight, down_weight) = args
    E, T = lax.axis_size("ep"), lax.axis_size("tp")
    rows = queries.shape[0]
    heads = queries.shape[1] // HEAD
    erows, width = expert_tokens.shape
    part = width // T
    B = 2
    A = E // B
    bf16, f32 = jnp.bfloat16, jnp.float32
    V, DMA = pltpu.VMEM, pltpu.SemaphoreType.DMA
    vm = pl.BlockSpec(memory_space=pltpu.VMEM)
    hbm = pl.BlockSpec(memory_space=pltpu.HBM)

    operands = [
        queries, keys_values, forget_cache, heads_gain.reshape(1, -1), output_weight, expert_tokens,
        expert_gain.reshape(1, -1), routes.T, route_logits.T, gate_weight, up_weight, down_weight,
    ]
    small = [5, 6, 7, 8, 2, 3]
    lanes, half = 2 * HEAD, part // 2
    heads = heads // B

    def kernel(*refs):
        refs = list(refs)
        load_sem = refs.pop()
        held = refs[-len(small) :]
        refs = refs[: -len(small)]
        loads = []
        for n, (index, place) in enumerate(zip(small, held)):
            loads.append(pltpu.make_async_copy(refs[index], place, load_sem.at[n]))
            refs[index] = place
        fused_kernel(E, T, loads, *refs)

    return pl.pallas_call(
        kernel,
        out_shape=(V((rows // T, output_weight.shape[1]), bf16), V((erows, part), bf16)),
        in_specs=[hbm] * len(operands),
        out_specs=(vm, vm),
        scratch_shapes=[
            V(output_weight.shape, bf16),
            V(gate_weight.shape[1:], bf16),
            V(up_weight.shape[1:], bf16),
            V(down_weight.shape[1:], bf16),
            V((T, E, erows, part), bf16),
            V((B, rows, lanes), bf16),
            V((B, rows, lanes), bf16),
            V((rows, lanes), bf16),
            V((rows, lanes), bf16),
            V((A, 2 * rows, lanes), bf16),
            V((heads, B, B, rows, 2 * lanes), bf16),
            V((E * rows, lanes), bf16),
            V((heads, B, 1, rows), f32),
            V((heads, B, HEAD + 16, rows), f32),
            V((A, 2, 2, B, erows, half), bf16),
            V((A, 2, 2, B, erows, half), bf16),
            V((A, 2, 2, B, erows, half), bf16),
            V((A, 2, 2, erows, half), bf16),
            V((A, 2, 2, erows, half), bf16),
            V((A, 2, erows, half), bf16),
            V((A, 2, erows, half), bf16),
            V((A, 2, erows, half), bf16),
            V((A, 2, erows, half), bf16),
            V((E, E, erows), f32),
            V((B, T, rows // T, lanes), bf16),
            V((T, B, rows // T, lanes), bf16),
            DMA((8,)),
            DMA((SEND_SLOTS,)),
            DMA((E, T)),
            DMA((E,)),
            DMA((1,)),
            DMA((1,)),
            DMA((A,)),
            DMA((A, 2)),
            DMA((A, 2)),
            DMA((A, 2)),
            DMA((A,)),
            DMA((E,)),
            DMA((T, B)),
        ]
        + [V(operands[n].shape, operands[n].dtype) for n in small]
        + [DMA((len(small),))],
        compiler_params=pltpu.CompilerParams(
            collective_id=0, has_side_effects=True, vmem_limit_bytes=60 * 1024 * 1024
        ),
    )(*operands)


def pick_body(*args):
    queries, keys_values, routes = args[0], args[1], args[7]
    rows, picks = routes.shape
    E, T = lax.axis_size("ep"), lax.axis_size("tp")
    capacity = 2 * rows * picks // E
    shapes = queries.shape[1] == 4 * HEAD and keys_values.shape[1] == 4 * HEAD
    if capacity >= rows and T == 4 and E == 8 and shapes:
        return fused_body(*args)
    return body(*args)


def solution(mesh):
    placed = (
        P("ep", "tp"),
        P("ep", "tp"),
        P("tp", None),
        P(),
        P(),
        P("ep", None),
        P(),
        P("ep", None),
        P("ep", None),
        P("ep", None, "tp"),
        P("ep", None, "tp"),
        P("ep", "tp", None),
    )
    return jax.shard_map(
        pick_body,
        mesh=mesh,
        in_specs=placed,
        out_specs=(P(("ep", "tp"), None), P("ep", "tp")),
        check_vma=False,
    )
```

```python
import math

import jax
import jax.numpy as jnp
from jax import lax
from jax.experimental import pallas as pl
from jax.experimental.pallas import tpu as pltpu
from jax.sharding import PartitionSpec as P

HEAD = 64


epsilon = 1e-06
clamp_limit = 7.0
sigmoid_slope = 1.702


def scaled_rows(values, gain_vector):
    as_float = values.astype(jnp.float32)
    inverse = lax.rsqrt(jnp.mean(as_float * as_float, axis=-1, keepdims=True) + epsilon)
    return (as_float * inverse * gain_vector).astype(jnp.bfloat16)


def assign_slots(routes, experts, capacity):
    row_count, pick_count = routes.shape
    flat_routes = routes.reshape(-1)
    onehot = (flat_routes[:, None] == jnp.arange(experts, dtype=jnp.int32)[None, :]).astype(
        jnp.int32
    )
    earlier = jnp.cumsum(onehot, axis=0) - onehot
    slot_rank = jnp.sum(earlier * onehot, axis=1)
    position = flat_routes * capacity + slot_rank
    owner_row = jnp.arange(row_count * pick_count, dtype=jnp.int32) // pick_count
    slot_token = jnp.full((experts * capacity,), row_count, jnp.int32).at[position].set(owner_row)
    return (position.reshape(row_count, pick_count), slot_token)


def body(
    queries,
    keys_values,
    forget_cache,
    heads_gain,
    output_weight,
    expert_tokens,
    expert_gain,
    routes,
    route_logits,
    gate_weight,
    up_weight,
    down_weight,
):
    row_count = queries.shape[0]
    query_count = queries.shape[1] // HEAD
    key_count = keys_values.shape[1] // (2 * HEAD)
    group_size = query_count // key_count
    offset = lax.axis_index("ep") * row_count
    score_scale = 1.0 / math.sqrt(HEAD)
    count_rows = queries.shape[0]
    segment_positions = offset + jnp.arange(count_rows, dtype=jnp.int32)
    gate_rows = lax.dynamic_slice_in_dim(forget_cache, offset, count_rows, 1)
    segment_bias = gate_rows.T.reshape(count_rows, key_count, group_size, 1)
    segments = [
        (queries.reshape(count_rows, key_count, group_size, HEAD), segment_positions, segment_bias)
    ]
    start_states = tuple(
        [
            (
                jnp.full((grouped.shape[0], key_count, group_size), -jnp.inf, jnp.float32),
                jnp.zeros((grouped.shape[0], key_count, group_size), jnp.float32),
                jnp.zeros((grouped.shape[0], key_count, group_size, HEAD), jnp.float32),
            )
            for grouped, positions, bias in segments
        ]
    )
    piece_rows = lax.all_gather(
        keys_values.reshape(row_count, key_count, 2 * HEAD), "ep", axis=0, tiled=True
    )
    count_rows = piece_rows.shape[0]
    block_width = 512
    blocks = piece_rows.reshape(count_rows // block_width, block_width, key_count, 2 * HEAD)

    def one_block(states, scan_item):
        block_rows, block_index = scan_item
        first_key = block_index * block_width
        key_block = block_rows[:, :, :HEAD]
        value_block = block_rows[:, :, HEAD:]
        key_gate = lax.dynamic_slice_in_dim(forget_cache, first_key, block_width, 1).reshape(
            1, key_count, group_size, block_width
        )
        key_pos = first_key + jnp.arange(block_width, dtype=jnp.int32)
        updated = []
        for (grouped, positions, bias), state in zip(segments, states):

            def take_block(state_in, grouped=grouped, positions=positions, bias=bias):
                running_max, running_sum, weighted = state_in
                scores = (
                    jnp.einsum(
                        "qhgd,khd->qhgk", grouped, key_block, preferred_element_type=jnp.float32
                    )
                    * score_scale
                )
                scores = scores + bias - key_gate
                visible = (key_pos[None, :] <= positions[:, None])[:, None, None, :]
                scores = jnp.where(visible, scores, -jnp.inf)
                new_max = jnp.maximum(running_max, jnp.max(scores, axis=-1))
                safe_max = jnp.where(jnp.isfinite(new_max), new_max, 0.0)
                factor = jnp.exp(running_max - safe_max)
                weights = jnp.exp(scores - safe_max[..., None])
                running_sum = running_sum * factor + jnp.sum(weights, axis=-1)
                weighted = weighted * factor[..., None] + jnp.einsum(
                    "qhgk,khd->qhgd",
                    weights.astype(jnp.bfloat16),
                    value_block,
                    preferred_element_type=jnp.float32,
                )
                return (new_max, running_sum, weighted)

            def keep_state(state_in):
                return state_in

            updated.append(lax.cond(first_key <= positions[-1], take_block, keep_state, state))
        return (tuple(updated), None)

    final_states, _ = lax.scan(
        one_block, start_states, (blocks, jnp.arange(count_rows // block_width, dtype=jnp.int32))
    )
    outputs = [
        (weighted / running_sum[..., None])
        .reshape(running_sum.shape[0], query_count * HEAD)
        .astype(jnp.bfloat16)
        for running_max, running_sum, weighted in final_states
    ]
    attended = outputs[0]
    local_rows = lax.all_to_all(attended, "tp", split_axis=0, concat_axis=1, tiled=True)
    heads_normed = scaled_rows(local_rows, heads_gain)
    mixer_out = jnp.dot(heads_normed, output_weight, preferred_element_type=jnp.float32).astype(
        jnp.bfloat16
    )
    experts_count = lax.axis_size("ep")
    expert_rows, pick_count = routes.shape
    capacity = 2 * expert_rows * pick_count // experts_count
    expert_in = scaled_rows(expert_tokens, expert_gain)
    shifted = route_logits - jnp.max(route_logits, axis=1, keepdims=True)
    raised = jnp.exp(shifted)
    route_weight = raised / jnp.sum(raised, axis=1, keepdims=True)
    position, slot_token = assign_slots(routes, experts_count, capacity)
    model_width = expert_in.shape[1]
    part_width = model_width // lax.axis_size("tp")
    gate_local = gate_weight[0]
    up_local = up_weight[0]
    down_local = down_weight[0]
    own_columns = lax.dynamic_slice_in_dim(
        expert_in, lax.axis_index("tp") * part_width, part_width, 1
    )
    padded = jnp.concatenate([own_columns, jnp.zeros((1, part_width), jnp.bfloat16)], axis=0)
    outgoing = jnp.take(padded, slot_token, axis=0).reshape(experts_count, capacity, part_width)
    arrived = lax.all_to_all(outgoing, "ep", split_axis=0, concat_axis=0, tiled=True).reshape(
        experts_count * capacity, part_width
    )
    piece_rows = lax.all_gather(arrived, "tp", axis=1, tiled=True)
    gate_sum = jnp.dot(piece_rows, gate_local, preferred_element_type=jnp.float32)
    up_sum = jnp.dot(piece_rows, up_local, preferred_element_type=jnp.float32)
    gate_cut = jnp.minimum(gate_sum, clamp_limit)
    up_cut = jnp.clip(up_sum, -clamp_limit, clamp_limit)
    hidden = ((up_cut + 1.0) * gate_cut * jax.nn.sigmoid(sigmoid_slope * gate_cut)).astype(
        jnp.bfloat16
    )
    expert_out = lax.psum_scatter(
        lax.dot_general(
            down_local, hidden, (((0,), (1,)), ((), ())), preferred_element_type=jnp.float32
        ).astype(jnp.bfloat16),
        "tp",
        scatter_dimension=0,
        tiled=True,
    )
    returned = lax.all_to_all(expert_out, "ep", split_axis=1, concat_axis=1, tiled=True)
    picked = jnp.take(returned, position.reshape(-1), axis=1).reshape(
        part_width, expert_rows, pick_count
    )
    moe_out = jnp.einsum("crk,rk->rc", picked.astype(jnp.float32), route_weight).astype(
        jnp.bfloat16
    )
    return (mixer_out, moe_out)


MESH = pl.DeviceIdType.MESH
SEND_SLOTS = 88


def fused_kernel(
    E, T, loads,
    q_ref, kv_ref, f_ref, hg_ref, ow_hbm, tok_ref, eg_ref, routes_ref, logits_ref,
    gw_hbm, uw_hbm, dw_hbm,
    mix_ref, moe_ref,
    ow, gw, uw, dw, tokall, qraw, kvraw, qx, kvx, kvall, qa, fa, m_sc, acc_sc,
    s1s, s1r, s1o, s2s, s2r, s3s, s3r, zs, zr, wtab, att, attall,
    wsem, ssem, tok_rs, top_rs, qx_rs, kvx_rs, kv_rs, s1_rs, s2_rs, s3_rs, z_rs, wt_rs,
    att_rs,
):
    f32, bf16 = jnp.float32, jnp.bfloat16
    e = lax.axis_index("ep")
    t = lax.axis_index("tp")
    B = 2
    A = E // B
    a, b = e // B, e % B
    y, c = t // 2, t % 2
    mate = y * 2 + (1 - c)
    across_y = (1 - y) * 2 + c
    across_x = a * B + (1 - b)
    rows = q_ref.shape[0]
    heads = q_ref.shape[1] // HEAD // B
    erows, width = tok_ref.shape
    part = width // T
    half = part // 2
    lanes = 2 * HEAD
    extra = erows // 4
    loads = loads + [
        pltpu.make_async_copy(ref.at[:, g * lanes : (g + 1) * lanes], place.at[g], wsem.at[4 + 2 * n + g])
        for n, (ref, place) in enumerate(((kv_ref, kvraw), (q_ref, qraw)))
        for g in range(B)
    ]

    weight_copies = [
        pltpu.make_async_copy(gw_hbm.at[0], gw, wsem.at[0]),
        pltpu.make_async_copy(uw_hbm.at[0], uw, wsem.at[1]),
        pltpu.make_async_copy(dw_hbm.at[0], dw, wsem.at[2]),
        pltpu.make_async_copy(ow_hbm, ow, wsem.at[3]),
    ]
    for copy in loads:
        copy.start()

    barrier = pltpu.get_barrier_semaphore()
    for d in range(1, E):
        pl.semaphore_signal(barrier, inc=1, device_id=(lax.rem(e + d, E), t), device_id_type=MESH)
    for d in range(1, T):
        ot = lax.rem(t + d, T)
        pl.semaphore_signal(barrier, inc=1, device_id=(e, ot), device_id_type=MESH)
        pl.semaphore_signal(barrier, inc=1, device_id=(across_x, ot), device_id_type=MESH)

    for copy in loads[:4]:
        copy.wait()

    tokens = tok_ref[...].astype(f32)
    inverse = lax.rsqrt(jnp.mean(tokens * tokens, axis=-1, keepdims=True) + epsilon)
    in_rows = (tokens * inverse * eg_ref[...]).astype(bf16)
    for quarter in range(T):
        tokall[quarter, e] = in_rows[:, quarter * part : (quarter + 1) * part]
    logits = logits_ref[...]
    raised = jnp.exp(logits - jnp.max(logits, axis=0, keepdims=True))
    weight = raised / jnp.sum(raised, axis=0, keepdims=True)
    chosen = routes_ref[...]
    wtab[e] = jnp.concatenate(
        [jnp.sum(jnp.where(chosen == j, weight, 0.0), axis=0, keepdims=True) for j in range(E)],
        axis=0,
    )
    with jax.named_scope("barrier"):
        pl.semaphore_wait(barrier, E - 1 + 2 * (T - 1))

    sent, free = [], list(range(SEND_SLOTS))

    def send(cond, src, dst, recv, device):
        slot = free.pop(0)

        def build():
            return pltpu.make_async_remote_copy(
                src_ref=src, dst_ref=dst, send_sem=ssem.at[slot], recv_sem=recv,
                device_id=device, device_id_type=MESH,
            )

        sent.append((slot, cond, build))
        if cond is None:
            build().start()
        else:
            @pl.when(cond)
            def _():
                build().start()

    def retire(entries):
        for entry in list(entries):
            slot, cond, build = entry
            if cond is None:
                build().wait_send()
            else:
                @pl.when(cond)
                def _():
                    build().wait_send()
            sent.remove(entry)
            free.append(slot)

    def arrive(cond, dst, recv):
        def go():
            pltpu.make_async_remote_copy(
                src_ref=dst, dst_ref=dst, send_sem=ssem.at[0], recv_sem=recv,
                device_id=(e, mate), device_id_type=MESH,
            ).wait_recv()

        if cond is None:
            go()
        else:
            pl.when(cond)(go)

    def both(p, q):
        return q if p is None else (p if q is None else jnp.logical_and(p, q))

    def send_token_block(cond, j, up, down, across, own=False):
        pieces = [(tokall.at[t, j], tok_rs.at[j, t])]
        if not (up is False and down is False and across is False):
            pieces.append((tokall.at[across_y, j, :extra], top_rs.at[j]))
        for ref, recv in pieces:
            for go, inside, to in (
                (up, a + 1 < A, (e + B, t)),
                (down, a > 0, (e - B, t)),
                (across, None, (across_x, t)),
            ):
                if go is not False:
                    send(both(cond, both(None if go is True else go, inside)), ref, ref, recv, to)
        if not own:
            ref = tokall.at[t, j, extra:]
            send(cond, ref, ref, tok_rs.at[j, t], (e, across_y))
            ref = tokall.at[t, j]
            send(cond, ref, ref, tok_rs.at[j, t], (e, mate))

    def arrive_token(cond, j):
        arrive(cond, tokall.at[t, j], tok_rs.at[j, t])
        arrive(cond, tokall.at[across_y, j, :extra], top_rs.at[j])

    def y_forward(cond, j):
        arrive(cond, tokall.at[across_y, j, extra:], tok_rs.at[j, across_y])
        ref = tokall.at[across_y, j]
        send(cond, ref, ref, tok_rs.at[j, across_y], (e, mate))

    late = []

    def token_step(s):
        pending = list(late)
        late.clear()
        if s < A:
            up_ok, down_ok = a - s >= 0, a + s < A
            ju, jd = e - s * B, e + s * B
            arrive_token(up_ok, ju)
            send_token_block(up_ok, ju, True, False, a - s > 0)
            arrive_token(down_ok, jd)
            send_token_block(down_ok, jd, False, True, a + s < A - 1)
            late.extend([(up_ok, ju), (down_ok, jd)])
        if s <= A:
            for sign in (1, -1) if s > 1 else (0,):
                oa = a - sign * (s - 1)
                ok = None if s == 1 else (oa >= 0 if sign == 1 else oa < A)
                j = oa * B + (1 - b)
                arrive_token(ok, j)
                rise = oa == 0 if sign >= 0 else False
                fall = oa == A - 1 if sign <= 0 else False
                send_token_block(ok, j, rise, fall, False)
                late.append((ok, j))
        for cond, j in pending:
            y_forward(cond, j)

    def swap_kv():
        send(None, kvraw.at[1 - b], kvx, kvx_rs.at[0], (across_x, t))

    def swap_q():
        send(None, qraw.at[1 - b], qx, qx_rs.at[0], (across_x, t))

    def send_kv_row(cond, row):
        send(both(cond, a + 1 < A), kvall.at[row], kvall.at[row], kv_rs.at[row], (e + B, t))

    def kv_step(s):
        ok, row = a - s >= 0, a - s
        arrive(ok, kvall.at[row], kv_rs.at[row])
        send_kv_row(ok, row)

    def by_block(mine, other):
        return [jnp.where(b == 0, mine, other), jnp.where(b == 0, other, mine)]

    def pack_kv():
        arrive(None, kvx, kvx_rs.at[0])
        blocks = by_block(kvraw[b], kvx[...])
        kvall[a, :rows] = jnp.concatenate([block[:, :HEAD] for block in blocks], axis=1)
        values = jnp.concatenate([block[:, HEAD:] for block in blocks], axis=1)
        for n in range(rows // lanes):
            kvall[a, rows + n * lanes : rows + (n + 1) * lanes] = values[
                n * lanes : (n + 1) * lanes
            ].T
        send_kv_row(None, a)

    def pack_q():
        arrive(None, qx, qx_rs.at[0])
        zero = jnp.zeros((rows, HEAD), bf16)
        lane = lax.broadcasted_iota(jnp.int32, (rows, lanes), 1)
        for xb, block in enumerate(by_block(qraw[b], qx[...])):
            block = block * jnp.asarray(0.125, bf16)
            for h in range(heads):
                q = block[:, h * HEAD : (h + 1) * HEAD]
                chosen_lane = (lane == h) | (lane == h + 8) | (lane == h + 16)
                pick = jnp.where(chosen_lane, -1.0, 0.0).astype(bf16)
                for kb in range(B):
                    qa[h, xb, kb, :, :lanes] = jnp.concatenate(
                        [q, zero] if kb == 0 else [zero, q], axis=1
                    )
                    qa[h, xb, kb, :, lanes:] = pick

    def pack_gates():
        count = f_ref.shape[1]
        gates = f_ref[...]
        gates = jnp.where(b == 0, gates[:heads], gates[heads:])
        first = f_ref[:, pl.ds(pl.multiple_of(a * B * rows, rows), lanes)][:, :1]
        gates = gates - jnp.where(b == 0, first[:heads], first[heads:])
        high = gates.astype(bf16).astype(f32)
        rest = gates - high
        middle = rest.astype(bf16).astype(f32)
        low = rest - middle
        blank = jnp.zeros((8 - heads, count), f32)
        stack = jnp.concatenate(
            [high, blank, middle, blank, low, blank, jnp.zeros((lanes - 24, count), f32)], axis=0
        )
        for n in range(count // lanes):
            fa[n * lanes : (n + 1) * lanes] = stack[:, n * lanes : (n + 1) * lanes].T.astype(bf16)

    def attend(row, tiles):
        nc = rows // lanes

        def score(h, xb, kb, start):
            gate = fa[pl.ds(pl.multiple_of((row * B + kb) * rows, rows), rows)]
            lhs = jnp.concatenate([kvall[row, :rows], gate], axis=1)
            s = lax.dot_general(
                lhs, qa[h, xb, kb], (((1,), (1,)), ((), ())), preferred_element_type=f32
            )
            if start is not None and xb == kb:
                kp = lax.broadcasted_iota(jnp.int32, s.shape, 0)
                qp = lax.broadcasted_iota(jnp.int32, s.shape, 1)
                s = jnp.where(kp <= qp, s, -jnp.inf)
            return s

        def soften(h, xb, kb, start, s):
            top = jnp.max(s, axis=0, keepdims=True)
            factor = None
            if not start:
                old = m_sc[h, xb]
                top = jnp.maximum(top, old)
                factor = jnp.exp(old - top)
            m_sc[h, xb] = top
            return jnp.exp(s - top).astype(bf16), factor

        def gather(h, xb, kb, start, p, factor):
            vt = jnp.concatenate(
                [
                    kvall[row, rows + n * lanes + kb * HEAD : rows + n * lanes + (kb + 1) * HEAD]
                    for n in range(nc)
                ],
                axis=1,
            )
            lhs = jnp.concatenate([vt, jnp.ones((16, rows), bf16)], axis=0)
            pv = jnp.dot(lhs, p, preferred_element_type=f32)
            if not start:
                pv = acc_sc[h, xb] * factor + pv
            acc_sc[h, xb] = pv

        held, soft = {}, {}
        for i in range(len(tiles) + 2):
            if i < len(tiles):
                held[i] = score(*tiles[i])
            if 0 <= i - 1 < len(tiles):
                soft[i - 1] = soften(*tiles[i - 1], held.pop(i - 1))
            if 0 <= i - 2 < len(tiles):
                gather(*tiles[i - 2], *soft.pop(i - 2))

    def attend_own():
        tiles = [(h, xb, xb, True) for xb in range(B) for h in range(heads)]
        tiles += [(h, xb, kb, False) for xb in range(B) for kb in range(xb) for h in range(heads)]
        own = [(h, xb, kb, start) for h, xb, kb, start in tiles]
        attend(a, own)

    def up(s, xb):
        @pl.when(a - s >= 0)
        def _():
            with jax.named_scope("att"):
                attend(a - s, [(h, xb, kb, None) for kb in range(B) for h in range(heads)])

    crows = B * erows

    def chunk_z(i):
        if A == 4:
            return [a + 1 - 2 * (a % 2), (a + 2) % 4, 3 - a, a][i]
        return lax.rem(a + i + 1, A)

    def expert_chunk(i):
        start = chunk_z(i) * B
        mine = i == A - 1
        scale = []
        for k in range(B):
            for oy in range(2):
                quarter = oy * 2 + (1 - c)
                arrive(
                    (start + k != e) if mine else None,
                    tokall.at[quarter, start + k], tok_rs.at[start + k, quarter],
                )
            arrive((start + k != e) if mine else None, wtab.at[start + k], wt_rs.at[start + k])
            columns = wtab[start + k].T
            lane = lax.broadcasted_iota(jnp.int32, columns.shape, 1)
            scale.append(jnp.sum(jnp.where(lane == e, columns, 0.0), axis=1, keepdims=True))
        scale = jnp.concatenate(scale, axis=0)
        x = jnp.concatenate(
            [tokall[qt, pl.ds(start, B)].reshape(crows, part) for qt in range(T)], axis=1
        )
        gate = jnp.dot(x, gw[...], preferred_element_type=f32)
        up_sum = jnp.dot(x, uw[...], preferred_element_type=f32)
        gate = jnp.minimum(gate, clamp_limit)
        up_sum = jnp.clip(up_sum, -clamp_limit, clamp_limit)
        hidden = ((up_sum + 1.0) * gate * jax.nn.sigmoid(sigmoid_slope * gate)).astype(bf16)

        def down(oy, oc, place):
            col = pl.multiple_of((oy * 2 + oc) * part, part)
            out = jnp.dot(hidden, dw[:, pl.ds(col, part)], preferred_element_type=f32)
            out = (out * scale).astype(bf16)
            for n in range(2):
                place[n] = out[:, n * half : (n + 1) * half].reshape(B, erows, half)

        for p, oy in enumerate((1 - y, y)):
            down(oy, 1 - c, s1s.at[i, :, p])
        for n in range(2):
            send(None, s1s.at[i, n], s1r.at[i, n], s1_rs.at[i, n], (e, mate))
        for p, oy in enumerate((1 - y, y)):
            down(oy, c, s1o.at[i, :, p])

    def add(*terms):
        total = terms[0].astype(f32)
        for term in terms[1:]:
            total = total + term.astype(f32)
        return total.astype(bf16)

    def first_step(i):
        arrive(None, s1r.at[i, 0], s1_rs.at[i, 0])
        s2s[i, 0] = add(s1o[i, 0, 0], s1r[i, 0, 0])
        send(None, s2s.at[i, 0], s2r.at[i, 0], s2_rs.at[i, 0], (e, across_y))
        arrive(None, s1r.at[i, 1], s1_rs.at[i, 1])
        for p in range(2):
            s2s[i, 1, p] = add(s1o[i, 1, p, 1 - b], s1r[i, 1, p, 1 - b])
        send(None, s2s.at[i, 1], s2r.at[i, 1], s2_rs.at[i, 1], (across_x, t))

    def second_step(i):
        arrive(None, s2r.at[i, 0], s2_rs.at[i, 0])
        s3s[i, 0] = add(s1o[i, 0, 1, 1 - b], s1r[i, 0, 1, 1 - b], s2r[i, 0, 1 - b])
        send(None, s3s.at[i, 0], s3r.at[i, 0], s3_rs.at[i, 0], (across_x, t))
        arrive(None, s2r.at[i, 1], s2_rs.at[i, 1])
        s3s[i, 1] = add(s1o[i, 1, 0, b], s1r[i, 1, 0, b], s2r[i, 1, 0])
        send(None, s3s.at[i, 1], s3r.at[i, 1], s3_rs.at[i, 1], (e, across_y))

    def third_step(i):
        place = zr.at[a] if i == A - 1 else zs.at[i]
        arrive(None, s3r.at[i, 0], s3_rs.at[i, 0])
        place[0] = add(s1o[i, 0, 1, b], s1r[i, 0, 1, b], s2r[i, 0, b], s3r[i, 0])
        arrive(None, s3r.at[i, 1], s3_rs.at[i, 1])
        place[1] = add(s1o[i, 1, 1, b], s1r[i, 1, 1, b], s2r[i, 1, 1], s3r[i, 1])
        if i != A - 1:
            send(None, zs.at[i], zr.at[a], z_rs.at[a], (chunk_z(i) * B + b, t))

    def scoped(name, f, *args):
        with jax.named_scope(name):
            f(*args)

    send_token_block(None, e, True, True, True, own=True)
    for copy in loads[4:]:
        copy.wait()
    for copy in weight_copies:
        copy.start()
    for d in range(1, E):
        j = lax.rem(e + d, E)
        send(None, wtab.at[e], wtab.at[e], wt_rs.at[e], (j, t))

    arows = rows // T

    out_slots = [[free.pop(0) for _ in range(T)] for _ in range(B)]

    def out_copy(xb, d):
        ot = lax.rem(t + d, T)
        return pltpu.make_async_remote_copy(
            src_ref=att.at[xb, ot], dst_ref=attall.at[t, b], send_sem=ssem.at[out_slots[xb][d]],
            recv_sem=att_rs.at[t, b], device_id=(a * B + xb, ot), device_id_type=MESH,
        )

    def attention_out(row, xb):
        @pl.when(a == row)
        def _():
            with jax.named_scope("attout"):
                out = jnp.concatenate(
                    [acc_sc[h, xb, :HEAD] / acc_sc[h, xb, HEAD : HEAD + 1] for h in range(heads)],
                    axis=0,
                ).T.astype(bf16)
                for tt in range(T):
                    att[xb, tt] = out[tt * arows : (tt + 1) * arows]
                for d in range(1, T):
                    out_copy(xb, d).start()

                @pl.when(b == xb)
                def _():
                    attall[t, b] = att[xb, t]

                @pl.when(b != xb)
                def _():
                    out_copy(xb, 0).start()

    swap_kv()
    scoped("gates", pack_gates)
    scoped("tok1", token_step, 1)
    swap_q()
    scoped("tok2", token_step, 2)
    scoped("packkv", pack_kv)
    scoped("packq", pack_q)
    retire(sent[:14])
    scoped("own", attend_own)
    scoped("tok3", token_step, 3)
    for copy in weight_copies[:3]:
        copy.wait()
    retire(sent[:26])
    scoped("chunk0", expert_chunk, 0)
    scoped("tok4", token_step, 4)
    scoped("kv1", kv_step, 1)
    up(1, 0)
    scoped("r1_0", first_step, 0)
    scoped("tok5", token_step, 5)
    attention_out(0, 0)
    attention_out(0, 1)
    scoped("chunk1", expert_chunk, 1)
    up(1, 1)
    scoped("r1_1", first_step, 1)
    retire(sent[:44])
    scoped("kv2", kv_step, 2)
    scoped("r2_0", second_step, 0)
    scoped("chunk2", expert_chunk, 2)
    up(2, 0)
    scoped("r1_2", first_step, 2)
    attention_out(1, 0)
    attention_out(1, 1)
    scoped("chunk3", expert_chunk, 3)
    scoped("r2_1", second_step, 1)
    scoped("kv3", kv_step, 3)
    up(2, 1)
    scoped("r1_3", first_step, 3)
    scoped("r3_0", third_step, 0)
    attention_out(2, 0)
    attention_out(2, 1)
    scoped("r2_2", second_step, 2)

    up(3, 0)
    scoped("r3_1", third_step, 1)
    up(3, 1)
    scoped("r2_3", second_step, 3)
    scoped("r3_2", third_step, 2)
    attention_out(3, 0)
    attention_out(3, 1)
    scoped("r3_3", third_step, 3)
    weight_copies[3].wait()

    def mixer():
        for dx in range(B):
            for d in range(T):
                if dx or d:
                    ob, ot = lax.rem(b + dx, B), lax.rem(t + d, T)
                    arrive(None, attall.at[ot, ob], att_rs.at[ot, ob])
        mixed = jnp.concatenate(
            [attall[tt, bb] for tt in range(T) for bb in range(B)], axis=1
        ).astype(f32)
        inverse = lax.rsqrt(jnp.mean(mixed * mixed, axis=-1, keepdims=True) + epsilon)
        mixed = (mixed * inverse * hg_ref[...]).astype(bf16)
        mix_ref[...] = jnp.dot(mixed, ow[...], preferred_element_type=f32).astype(bf16)

    scoped("mixer", mixer)

    def combine():
        for d in range(1, A):
            oz = lax.rem(a + d, A)
            arrive(None, zr.at[oz], z_rs.at[oz])
        for n in range(2):
            moe_ref[:, n * half : (n + 1) * half] = add(*[zr[oz, n] for oz in range(A)])

    scoped("combine", combine)

    with jax.named_scope("drain"):
        retire(sent)
        for xb in range(B):
            for d in range(1, T):
                out_copy(xb, d).wait_send()

            @pl.when(b != xb)
            def _():
                out_copy(xb, 0).wait_send()


def fused_body(*args):
    (queries, keys_values, forget_cache, heads_gain, output_weight, expert_tokens,
     expert_gain, routes, route_logits, gate_weight, up_weight, down_weight) = args
    E, T = lax.axis_size("ep"), lax.axis_size("tp")
    rows = queries.shape[0]
    heads = queries.shape[1] // HEAD
    erows, width = expert_tokens.shape
    part = width // T
    B = 2
    A = E // B
    bf16, f32 = jnp.bfloat16, jnp.float32
    V, DMA = pltpu.VMEM, pltpu.SemaphoreType.DMA
    vm = pl.BlockSpec(memory_space=pltpu.VMEM)
    hbm = pl.BlockSpec(memory_space=pltpu.HBM)

    operands = [
        queries, keys_values, forget_cache, heads_gain.reshape(1, -1), output_weight, expert_tokens,
        expert_gain.reshape(1, -1), routes.T, route_logits.T, gate_weight, up_weight, down_weight,
    ]
    small = [5, 6, 7, 8, 2, 3]
    lanes, half = 2 * HEAD, part // 2
    heads = heads // B

    def kernel(*refs):
        refs = list(refs)
        load_sem = refs.pop()
        held = refs[-len(small) :]
        refs = refs[: -len(small)]
        loads = []
        for n, (index, place) in enumerate(zip(small, held)):
            loads.append(pltpu.make_async_copy(refs[index], place, load_sem.at[n]))
            refs[index] = place
        fused_kernel(E, T, loads, *refs)

    return pl.pallas_call(
        kernel,
        out_shape=(V((rows // T, output_weight.shape[1]), bf16), V((erows, part), bf16)),
        in_specs=[hbm] * len(operands),
        out_specs=(vm, vm),
        scratch_shapes=[
            V(output_weight.shape, bf16),
            V(gate_weight.shape[1:], bf16),
            V(up_weight.shape[1:], bf16),
            V(down_weight.shape[1:], bf16),
            V((T, E, erows, part), bf16),
            V((B, rows, lanes), bf16),
            V((B, rows, lanes), bf16),
            V((rows, lanes), bf16),
            V((rows, lanes), bf16),
            V((A, 2 * rows, lanes), bf16),
            V((heads, B, B, rows, 2 * lanes), bf16),
            V((E * rows, lanes), bf16),
            V((heads, B, 1, rows), f32),
            V((heads, B, HEAD + 16, rows), f32),
            V((A, 2, 2, B, erows, half), bf16),
            V((A, 2, 2, B, erows, half), bf16),
            V((A, 2, 2, B, erows, half), bf16),
            V((A, 2, 2, erows, half), bf16),
            V((A, 2, 2, erows, half), bf16),
            V((A, 2, erows, half), bf16),
            V((A, 2, erows, half), bf16),
            V((A, 2, erows, half), bf16),
            V((A, 2, erows, half), bf16),
            V((E, E, erows), f32),
            V((B, T, rows // T, lanes), bf16),
            V((T, B, rows // T, lanes), bf16),
            DMA((8,)),
            DMA((SEND_SLOTS,)),
            DMA((E, T)),
            DMA((E,)),
            DMA((1,)),
            DMA((1,)),
            DMA((A,)),
            DMA((A, 2)),
            DMA((A, 2)),
            DMA((A, 2)),
            DMA((A,)),
            DMA((E,)),
            DMA((T, B)),
        ]
        + [V(operands[n].shape, operands[n].dtype) for n in small]
        + [DMA((len(small),))],
        compiler_params=pltpu.CompilerParams(
            collective_id=0, has_side_effects=True, vmem_limit_bytes=60 * 1024 * 1024
        ),
    )(*operands)


def pick_body(*args):
    queries, keys_values, routes = args[0], args[1], args[7]
    rows, picks = routes.shape
    E, T = lax.axis_size("ep"), lax.axis_size("tp")
    capacity = 2 * rows * picks // E
    shapes = queries.shape[1] == 4 * HEAD and keys_values.shape[1] == 4 * HEAD
    if capacity >= rows and T == 4 and E == 8 and shapes:
        return fused_body(*args)
    return body(*args)


def solution(mesh):
    placed = (
        P("ep", "tp"),
        P("ep", "tp"),
        P("tp", None),
        P(),
        P(),
        P("ep", None),
        P(),
        P("ep", None),
        P("ep", None),
        P("ep", None, "tp"),
        P("ep", None, "tp"),
        P("ep", "tp", None),
    )
    return jax.shard_map(
        pick_body,
        mesh=mesh,
        in_specs=placed,
        out_specs=(P(("ep", "tp"), None), P("ep", "tp")),
        check_vma=False,
    )
```
